128 devices in a mesh: kv: 16 (over z, y), tp: 8 (over x, core).
Axes of the slice: x: 4, y: 4, z: 4, core: 2. Of those that a mesh axis runs over, the one named last changes fastest.
Arguments:
- tokens: bfloat16 [48, 24, 4096], P(None, None, 'kv'), may hold values from -6 to 6
- norm_gain: bfloat16 [4096], P('kv'), may hold values from 0.099609375 to 1.8984375
- w_query: bfloat16 [4096, 2048], P('kv', 'tp'), may hold values from -0.09375 to 0.09375
- w_key: bfloat16 [4096, 512], P('kv', 'tp'), may hold values from -0.09375 to 0.09375
- w_value: bfloat16 [4096, 512], P('kv', 'tp'), may hold values from -0.09375 to 0.09375
- w_forget: bfloat16 [4096, 32], replicated, may hold values from -0.09375 to 0.09375
- forget_bias: float32 [32], P('tp'), may hold values from -1 to 3
- query_gain: bfloat16 [64], replicated, may hold values from 0.099609375 to 1.8984375
- key_gain: bfloat16 [64], replicated, may hold values from 0.099609375 to 1.8984375
- w_out: bfloat16 [2048, 4096], P('tp', 'kv'), may hold values from -0.5 to 0.5
- key_cache: bfloat16 [48, 512, 16384], P(None, 'tp', 'kv'), may hold values from -46 to 46
- value_cache: bfloat16 [48, 512, 16384], P(None, 'tp', 'kv'), may hold values from -6 to 6
- gate_sums: float32 [48, 32, 16384], P(None, 'tp', 'kv'), may hold values from -2051 to 0, as said below
- parents: int32 [48, 24], replicated, may hold values from -1 to 22, as said below
- lengths: int32 [48], replicated, may hold values from 8192 to 16378
- accepted: int32 [48], replicated, may hold values from 0 to 6
Outputs:
- mixed: bfloat16 [48, 24, 4096], P(None, None, 'kv')
The draws below stay inside these ranges and needn't reach their ends.
Inputs may be any that keep to these rules, and one draw needn't show every extreme that they name: `gate_sums`: for each sequence and head it never rises along the positions. `parents`: the parent of proposal i is -1 (the cache's last visible position) or one of the proposals i - 3 to i - 1. The accepted proposals stand in the cache right after the first lengths positions.
All inputs are finite; a program needn't handle non-finite values.
Results may differ from the reference program's by a relative error of at most 0.03.
Values may be sent and summed in bfloat16 or wider, within the bound.
A program may use at most 128 MiB of HBM per device.

```python
import jax
import jax.numpy as jnp
from jax import lax

D = 4096
HEADS = 32
KV_HEADS = 8
HEAD_DIM = 64
DRAFT = 24
POS_DEV = 1024
BATCH = 48
LENGTH = 16384
N_TP = 8


def draw_key_cache(key, part):
    base_key, sign_key = jax.random.split(jax.random.fold_in(key, 37), 2)
    noise = jnp.clip(jax.random.normal(base_key, (BATCH, KV_HEADS * HEAD_DIM, LENGTH), jnp.float32), -6.0, 6.0)
    signs = jnp.where(jax.random.bernoulli(sign_key, 0.5, (KV_HEADS * HEAD_DIM,)), 1.0, -1.0)
    first_row = (jnp.arange(BATCH, dtype=jnp.int32) == 0).astype(jnp.float32)
    shift = 40.0 * first_row[:, None, None] * signs[None, :, None]
    return (noise + shift).astype(jnp.bfloat16)


def draw_lengths(key, part):
    low = LENGTH // 2
    span = LENGTH - DRAFT // 4 - low + 1
    picks = jax.random.randint(jax.random.fold_in(key, 41), (BATCH,), 0, span)
    row_ids = jnp.arange(BATCH, dtype=jnp.int32)
    spread = jnp.where(row_ids == 1, picks[0] + span // 2, picks)
    return (low + spread % span).astype(jnp.int32)


def draw_gate_sums(key, part):
    pick_key, fast_key, slow_key, block_key, rough_key, spot_key, loss_key = jax.random.split(jax.random.fold_in(key, 11), 7)
    order = jax.random.permutation(pick_key, HEADS)
    fast_heads = order < HEADS // 2
    fast_rate = jnp.exp(jax.random.uniform(fast_key, (BATCH, HEADS), jnp.float32, jnp.log(1.0 / 50.0), jnp.log(1.0 / 30.0)))
    slow_rate = jax.random.uniform(slow_key, (BATCH, HEADS), jnp.float32, 0.5, 2.0) / LENGTH
    base_rate = jnp.where(fast_heads[None, :], fast_rate, slow_rate)
    block_factor = jnp.exp(jax.random.uniform(block_key, (BATCH, HEADS, LENGTH // POS_DEV), jnp.float32, jnp.log(0.4), jnp.log(2.5)))
    block_factor = jnp.repeat(block_factor, POS_DEV, axis=2)
    rough = jax.random.uniform(rough_key, (BATCH, HEADS, LENGTH), jnp.float32, 0.5, 1.5)
    gate_logarithm = -base_rate[:, :, None] * block_factor * rough
    cache_positions = jax.random.randint(spot_key, (BATCH, 3), 0, LENGTH)
    loss_values = jax.random.uniform(loss_key, (BATCH, HEADS, 3), jnp.float32, 0.2, 0.5)
    slot_positions = jnp.arange(LENGTH, dtype=jnp.int32)
    for draft_group_index in range(3):
        match_flag = slot_positions[None, None, :] == cache_positions[:, None, draft_group_index:draft_group_index + 1]
        gate_logarithm = gate_logarithm + jnp.where(match_flag, jnp.log(1.0 - loss_values[:, :, draft_group_index:draft_group_index + 1]), 0.0)
    return jnp.cumsum(gate_logarithm, axis=2)


def draw_parents(key, part):
    node_ids = jnp.arange(DRAFT, dtype=jnp.int32)
    step_back = jax.random.randint(jax.random.fold_in(key, 23), (BATCH, DRAFT), 1, 4)
    return jnp.maximum(node_ids[None, :] - step_back, -1).astype(jnp.int32)


def plant(entries, own_key, smallest, top_value):
    shape = entries.shape
    spot = [jax.random.randint(jax.random.fold_in(own_key, axis), (), 0, shape[axis]) for axis in range(len(shape))]
    entries = entries.at[tuple(spot)].set(smallest)
    longest = shape.index(max(shape))
    spot[longest] = (spot[longest] + 1) % shape[longest]
    return entries.at[tuple(spot)].set(top_value)


def block_levels(key, shape, cuts, smallest, high):
    factor_of, own = 1.0, jax.random.fold_in(key, 6)
    for axis_at, shards_of in cuts:
        heights = jnp.exp(jax.random.uniform(jax.random.fold_in(own, axis_at), (shards_of,), jnp.float32, smallest / len(cuts), high / len(cuts)))
        factor_of = factor_of * jnp.repeat(heights, shape[axis_at] // shards_of).reshape([-1 if axis == axis_at else 1 for axis in range(len(shape))])
    return factor_of


def scatter_about(stream_key, extent, width, bound, cuts=(), kind=jnp.bfloat16):
    values = jax.random.normal(stream_key, extent, jnp.float32) * width
    if len(cuts) > 0:
        values = block_levels(stream_key, extent, cuts, -0.22, 0.18) * values
    return jnp.clip(values, min=-bound, max=bound).astype(kind)


def setup_inputs(seed: int = 0) -> dict:
    key_list = jax.random.split(jax.random.key(seed), 17)
    tokens = scatter_about(key_list[0], (BATCH, DRAFT, D), 1.0, 6.0, ((2, 16),))
    norm_gain = jnp.clip(1.0 + 0.18 * jax.random.normal(key_list[1], (D,), jnp.float32), 0.099609375, 1.8984375).astype(jnp.bfloat16)
    w_query = scatter_about(key_list[2], (D, HEADS * HEAD_DIM), D ** -0.5, 0.09375, ((0, 16), (1, 8)))
    w_key = scatter_about(key_list[3], (D, KV_HEADS * HEAD_DIM), D ** -0.5, 0.09375, ((0, 16), (1, 8)))
    w_value = scatter_about(key_list[4], (D, KV_HEADS * HEAD_DIM), D ** -0.5, 0.09375, ((0, 16), (1, 8)))
    w_forget = scatter_about(key_list[5], (D, HEADS), D ** -0.5, 0.09375)
    forget_bias = jnp.clip(-1.0 + 4.0 * jax.random.uniform(key_list[6], (HEADS,), jnp.float32) ** block_levels(key_list[6], (HEADS,), ((0, 8),), -0.2, 0.2), -1.0, 3.0)
    query_gain = jnp.clip(1.0 + 0.18 * jax.random.normal(key_list[7], (HEAD_DIM,), jnp.float32), 0.099609375, 1.8984375).astype(jnp.bfloat16)
    key_gain = jnp.clip(1.0 + 0.18 * jax.random.normal(key_list[8], (HEAD_DIM,), jnp.float32), 0.099609375, 1.8984375).astype(jnp.bfloat16)
    w_out = scatter_about(key_list[9], (HEADS * HEAD_DIM, D), (2 * HEAD_DIM) ** -0.5, 0.5, ((0, 8), (1, 16)))
    key_cache = draw_key_cache(jax.random.fold_in(key_list[16], 71), 0)
    value_cache = scatter_about(key_list[11], (BATCH, KV_HEADS * HEAD_DIM, LENGTH), 1.0, 6.0, ((1, 8), (2, 16)))
    gate_sums = draw_gate_sums(jax.random.fold_in(key_list[16], 71), 0)
    parents = draw_parents(jax.random.fold_in(key_list[16], 71), 0)
    lengths = draw_lengths(jax.random.fold_in(key_list[16], 71), 0)
    accepted = plant(jax.random.randint(key_list[15], (BATCH,), 0, DRAFT // 4 + 1), jax.random.fold_in(key_list[15], 1), 0, (DRAFT // 4 + 1) - 1).astype(jnp.int32)
    return dict(tokens=tokens, norm_gain=norm_gain, w_query=w_query, w_key=w_key, w_value=w_value, w_forget=w_forget, forget_bias=forget_bias, query_gain=query_gain, key_gain=key_gain, w_out=w_out, key_cache=key_cache, value_cache=value_cache, gate_sums=gate_sums, parents=parents, lengths=lengths, accepted=accepted)


eps = 1e-05

def head_norm(block, gain):
    mean_sq = lax.optimization_barrier(jnp.mean(block * block, axis=-1, keepdims=True))
    return (block * lax.rsqrt(mean_sq + eps) * gain.astype(jnp.float32)).astype(jnp.bfloat16)

def ancestors(parents, node_count):
    node_ids = jnp.arange(node_count, dtype=jnp.int32)
    reach_map = (parents[:, :, None] == node_ids[None, None, :]).astype(jnp.float32)
    reach_map = reach_map + jnp.eye(node_count, dtype=jnp.float32)[None]
    for repeat_index in range(max(node_count - 1, 1).bit_length()):
        reach_map = jnp.minimum(jnp.einsum('bij,bjk->bik', reach_map, reach_map, precision=lax.Precision.HIGHEST), 1.0)
    return reach_map

def reference(tokens, norm_gain, w_query, w_key, w_value, w_forget, forget_bias, query_gain, key_gain, w_out, key_cache, value_cache, gate_sums, parents, lengths, accepted):
    row_count = BATCH * DRAFT
    group_size = HEADS // KV_HEADS
    scale = HEAD_DIM ** (-0.5)
    wide_rows = tokens.reshape(row_count, D).astype(jnp.float32)
    squares = lax.optimization_barrier(jnp.sum(wide_rows * wide_rows, axis=1))
    inverse = lax.rsqrt(squares / D + eps)
    scaled = (wide_rows * norm_gain.astype(jnp.float32)[None, :]).astype(jnp.bfloat16)

    def project(weight):
        return jnp.dot(scaled, weight, preferred_element_type=jnp.float32) * inverse[:, None]
    query_rows = lax.optimization_barrier(head_norm(project(w_query).reshape(BATCH, DRAFT, HEADS, HEAD_DIM), query_gain))
    keys_new = lax.optimization_barrier(head_norm(project(w_key).reshape(BATCH, DRAFT, KV_HEADS, HEAD_DIM), key_gain))
    values_new = lax.optimization_barrier(project(w_value).astype(jnp.bfloat16)).reshape(BATCH, DRAFT, KV_HEADS, HEAD_DIM)
    gate_logarithm = jax.nn.log_sigmoid(project(w_forget) + forget_bias.astype(jnp.float32)[None, :]).reshape(BATCH, DRAFT, HEADS)
    reach_map = ancestors(parents, DRAFT)
    path_sums = jnp.einsum('bij,bjh->bhi', reach_map, gate_logarithm, precision=lax.Precision.HIGHEST)
    valid_len = lengths + accepted
    slot_positions = jnp.arange(LENGTH, dtype=jnp.int32)

    def one_sequence(items):
        query_seq, key_new, value_new, key_seq, value_seq, gate_seq, path_seq, reach_seq, length_now = items
        query_wide = query_seq.astype(jnp.float32).reshape(DRAFT, KV_HEADS, group_size, HEAD_DIM)
        key_wide = key_seq.astype(jnp.float32).reshape(KV_HEADS, HEAD_DIM, LENGTH)
        gate_last = lax.optimization_barrier(jnp.sum(jnp.where(slot_positions[None, :] == length_now - 1, gate_seq, 0.0), axis=1))
        cache_logits = jnp.einsum('pkgd,kds->kgps', query_wide, key_wide).reshape(HEADS, DRAFT, LENGTH)
        cache_logits = cache_logits * scale + (gate_last[:, None] + path_seq)[:, :, None] - gate_seq[:, None, :]
        cache_logits = jnp.where((slot_positions < length_now)[None, None, :], cache_logits, -jnp.inf)
        new_logits = jnp.einsum('pkgd,jkd->kgpj', query_wide, key_new.astype(jnp.float32)).reshape(HEADS, DRAFT, DRAFT)
        new_logits = new_logits * scale + path_seq[:, :, None] - path_seq[:, None, :]
        new_logits = jnp.where((reach_seq > 0.5)[None], new_logits, -jnp.inf)
        weights = jax.nn.softmax(jnp.concatenate([cache_logits, new_logits], axis=2), axis=2).astype(jnp.bfloat16)
        weights = lax.optimization_barrier(weights).astype(jnp.float32)
        value_rows = jnp.transpose(value_seq.reshape(KV_HEADS, HEAD_DIM, LENGTH), (2, 0, 1))
        value_all = jnp.concatenate([value_rows, value_new], axis=0).astype(jnp.float32)
        attended = jnp.einsum('kgps,skd->pkgd', weights.reshape(KV_HEADS, group_size, DRAFT, LENGTH + DRAFT), value_all)
        return attended.reshape(DRAFT, HEADS * HEAD_DIM).astype(jnp.bfloat16)
    attended = lax.map(one_sequence, (query_rows, keys_new, values_new, key_cache, value_cache, gate_sums, path_sums, reach_map, valid_len))
    attended = lax.optimization_barrier(attended).reshape(row_count, HEADS * HEAD_DIM)
    group_width = HEADS * HEAD_DIM // N_TP
    summed = jnp.zeros((row_count, D), jnp.float32)
    for group_index in range(N_TP):
        group_part = jnp.dot(attended[:, group_index * group_width:(group_index + 1) * group_width], w_out[group_index * group_width:(group_index + 1) * group_width], preferred_element_type=jnp.float32)
        summed = summed + lax.optimization_barrier(group_part.astype(jnp.bfloat16)).astype(jnp.float32)
    return summed.astype(jnp.bfloat16).reshape(BATCH, DRAFT, D)
```

```python
import functools

import jax
import jax.numpy as jnp
from jax import lax
from jax.experimental import pallas as pl
from jax.experimental.pallas import tpu as pltpu
from jax.sharding import PartitionSpec as P

f32, bf16 = jnp.float32, jnp.bfloat16
eps = 1e-05
floor_value = -1e30
KV_SIDE = 4
N_KV = 16
N_TP = 8
MESH = pl.DeviceIdType.MESH

PROJ, STAT, QUERY, PART, LSE, ATT, OUT, FINAL = range(8)


def dot(a, b):
    return jnp.dot(a, b, preferred_element_type=f32)


def dot_nt(a, b):
    return lax.dot_general(a, b, (((1,), (1,)), ((), ())), preferred_element_type=f32)


def halves(value):
    high = value.astype(bf16)
    return high, (value - high.astype(f32)).astype(bf16)


def padded(value, rows):
    return jnp.concatenate([value, jnp.zeros((rows - value.shape[0], value.shape[1]), value.dtype)], axis=0)


def lanes(shape):
    return lax.broadcasted_iota(jnp.int32, shape, 1)


def rows_of(shape):
    return lax.broadcasted_iota(jnp.int32, shape, 0)


def kernel(
    tokens, norm_gain, w_query, w_key, w_value, w_forget, forget_bias, query_gain, key_gain, w_out,
    key_cache, value_cache, gate_sums, parents, lengths, accepted,
    out,
    w_all, wf, keys, values, gates, reach, p_send, p_recv, s_send, s_recv, own_proj, q_all, kv_new,
    path_tile, o_send, o_recv, l_send, l_recv, a_all, t_send, t_recv, fin,
    local_sem, send_sem, recv_sem,
):
    kv = lax.axis_index("kv")
    tp = lax.axis_index("tp")
    z, y = kv // KV_SIDE, kv % KV_SIDE
    x, core = tp // 2, tp % 2
    share = q_all.shape[1]
    seqs = 3
    drafts = share // seqs
    heads = 4
    head_dim = 64
    width = heads * head_dim
    positions = key_cache.shape[2]
    model_width = w_forget.shape[0]

    def ahead(o):
        return ((z + o // KV_SIDE) % KV_SIDE) * KV_SIDE + (y + o % KV_SIDE) % KV_SIDE

    def behind(o):
        return ((z + KV_SIDE - o // KV_SIDE) % KV_SIDE) * KV_SIDE + (y + KV_SIDE - o % KV_SIDE) % KV_SIDE

    def tp_ahead(u):
        return ((x + u // 2) % 4) * 2 + (core + u) % 2

    def remote(kind, index, src, dst, device):
        return pltpu.make_async_remote_copy(
            src_ref=src, dst_ref=dst, send_sem=send_sem.at[kind, index], recv_sem=recv_sem.at[kind, index],
            device_id=device, device_id_type=MESH,
        )

    barrier = pltpu.get_barrier_semaphore()
    for o in range(1, N_KV):
        pl.semaphore_signal(barrier, inc=1, device_id={"kv": ahead(o)}, device_id_type=MESH)
    for u in range(1, N_TP):
        pl.semaphore_signal(barrier, inc=1, device_id={"tp": tp_ahead(u)}, device_id_type=MESH)

    wf_copy = pltpu.make_async_copy(w_forget.at[pl.ds(kv * 256, 256)], wf, local_sem.at[0])
    gate_copy = pltpu.make_async_copy(gate_sums, gates, local_sem.at[1])
    key_copy = pltpu.make_async_copy(key_cache, keys, local_sem.at[2])
    value_copy = pltpu.make_async_copy(value_cache, values, local_sem.at[3])
    wf_copy.start()
    gate_copy.start()
    key_copy.start()
    value_copy.start()

    w_all[:, :width] = w_query[...]
    w_all[:, width:] = jnp.concatenate([w_key[...].astype(f32), w_value[...].astype(f32)], axis=1).astype(bf16)
    wf_copy.wait()
    gate_copy.wait()
    pick = (lanes((8, 32)) == rows_of((8, 32)) + 4 * tp) & (rows_of((8, 32)) < 4)
    gate_weights = dot_nt(pick.astype(f32).astype(bf16), wf[...]).astype(bf16)
    square_row = (rows_of((8, 256)) == 4).astype(f32).astype(bf16)
    gain = norm_gain[...].astype(f32)
    place = lanes((heads, positions)) + kv * positions
    tile_lane = lanes((8, 128))
    tile_row = rows_of((8, 128))

    def project(o, carry):
        chunk = ahead(o)
        wide = padded(tokens[chunk].astype(f32), 128)
        scaled = (wide * gain).astype(bf16)
        high, low = halves(wide * wide)
        tile = dot_nt(gate_weights, scaled) + dot_nt(square_row, high) + dot_nt(square_row, low)
        for j in range(seqs):
            b = chunk * seqs + j
            last = jnp.sum(
                jnp.where(place == lengths[b] + accepted[b] - 1, gates[b], 0.0), axis=1, keepdims=True
            )
            last = jnp.concatenate([last, jnp.zeros((4, 1), f32)], axis=0)
            tile = jnp.where(tile_lane == share + j, last, tile)
        s_send[o] = tile
        projected = dot(scaled, w_all[...])[:share]
        p_send[o] = projected.astype(bf16)
        own_proj[...] = projected
        return carry

    lax.fori_loop(0, N_KV, lambda i, c: project(N_KV - 1 - i, c), 0)

    pl.semaphore_wait(barrier, N_KV + N_TP - 2)
    for o in range(1, N_KV):
        remote(STAT, o, s_send.at[o], s_recv.at[o], {"kv": ahead(o)}).start()
        remote(PROJ, o, p_send.at[o], p_recv.at[o], {"kv": ahead(o)}).start()

    row_lane = lanes((1, 128))
    for j in range(seqs):
        for p in range(drafts):
            parent = parents[kv * seqs + j, p]
            at = jnp.where(parent >= 0, parent + drafts * j, -1)
            i = drafts * j + p
            reach[i : i + 1, :] = ((row_lane == i) | (row_lane == at)).astype(f32)
    reach[share:, :] = jnp.zeros((128 - share, 128), f32)
    closure = reach[...]
    for _ in range(5):
        closure = jnp.minimum(dot(closure.astype(bf16), closure.astype(bf16)), 1.0)
    reach[...] = closure

    head_of = lax.broadcasted_iota(jnp.int32, (384, 384), 0) // head_dim
    head_at = lax.broadcasted_iota(jnp.int32, (384, 384), 1) // head_dim
    head_mean = jnp.where(head_of == head_at, 1.0 / head_dim, 0.0).astype(bf16)
    gains = jnp.concatenate([query_gain[...].astype(f32)] * 4 + [key_gain[...].astype(f32)] * 2, axis=1)

    def add_in(o, carry):
        total, stats = carry
        remote(STAT, o, s_send.at[o], s_recv.at[o], {"kv": ahead(o)}).wait_recv()
        remote(PROJ, o, p_send.at[o], p_recv.at[o], {"kv": ahead(o)}).wait_recv()
        return total + p_recv[o].astype(f32), stats + s_recv[o]

    total, stats = lax.fori_loop(1, N_KV, add_in, (own_proj[...], s_send[0]))
    inverse_tile = lax.rsqrt(stats / model_width + eps)
    inverse = jnp.concatenate([inverse_tile] * 16, axis=0).T[:share, 4:5]
    total = total * inverse
    high, low = halves(total * total)
    mean_sq = dot(high, head_mean) + dot(low, head_mean)
    normed = total * lax.rsqrt(mean_sq + eps) * gains
    q_all[0] = (normed[:, :width].astype(bf16).astype(f32) * head_dim ** (-0.5)).astype(bf16)
    for o in range(1, N_KV):
        remote(QUERY, o, q_all.at[0], q_all.at[o], {"kv": ahead(o)}).start()
    kv_new[...] = jnp.concatenate([normed[:, width : width + head_dim], total[:, width + head_dim :]], axis=1)

    bias = jnp.where(
        tile_row == 0, forget_bias[0],
        jnp.where(tile_row == 1, forget_bias[1], jnp.where(tile_row == 2, forget_bias[2], forget_bias[3])),
    )
    gate_pre = stats * inverse_tile[4:5, :] + bias
    log_gate = jnp.minimum(gate_pre, 0.0) - jnp.log1p(jnp.exp(-jnp.abs(gate_pre)))
    log_gate = jnp.where(tile_lane < share, log_gate, 0.0)
    top_part, rest = halves(log_gate)
    left = log_gate - top_part.astype(f32)
    middle, last_part = halves(left)
    follows = reach[...].astype(bf16)
    path = dot_nt(top_part, follows) + dot_nt(middle, follows) + dot_nt(last_part, follows)
    last_gate = jnp.where(
        tile_lane < drafts, stats[:, share : share + 1],
        jnp.where(tile_lane < 2 * drafts, stats[:, share + 1 : share + 2], stats[:, share + 2 : share + 3]),
    )
    path_tile[...] = path + last_gate

    key_copy.wait()
    value_copy.wait()
    wide_lane = lanes((heads * drafts, 128))

    def attend(o, carry):
        src = behind(o)

        @pl.when(o > 0)
        def _():
            remote(QUERY, o, q_all.at[0], q_all.at[o], {"kv": ahead(o)}).wait_recv()

        queries = q_all[o].astype(f32)
        pieces, sums = [], jnp.zeros((heads * drafts, 128), f32)
        for j in range(seqs):
            b = src * seqs + j
            block = queries[j * drafts : (j + 1) * drafts]
            stacked = jnp.concatenate(
                [block[:, h * head_dim : (h + 1) * head_dim] for h in range(heads)], axis=0
            ).astype(bf16)
            logits = dot(stacked, keys[b])
            kept = jnp.where(place < lengths[b] + accepted[b], -gates[b], floor_value)
            tops, weights, totals = [], [], []
            for h in range(heads):
                row = logits[h * drafts : (h + 1) * drafts] + kept[h : h + 1]
                top = jnp.max(row, axis=1, keepdims=True)
                weight = jnp.exp(row - top)
                tops.append(top)
                weights.append(weight)
                totals.append(jnp.sum(weight, axis=1, keepdims=True))
            weighted = dot_nt(jnp.concatenate(weights, axis=0).astype(bf16), values[b])
            all_total = jnp.concatenate(totals, axis=0)
            weighted = weighted / all_total
            sums = jnp.where(wide_lane == j, jnp.concatenate(tops, axis=0) + jnp.log(all_total), sums)
            pieces.append(
                jnp.concatenate([weighted[h * drafts : (h + 1) * drafts] for h in range(heads)], axis=1)
            )
        o_send[o] = jnp.concatenate(pieces, axis=0).astype(bf16)
        l_send[o] = padded(sums, 128).T[:8]

        @pl.when(o > 0)
        def _():
            remote(LSE, o, l_send.at[o], l_recv.at[o], {"kv": src}).start()
            remote(PART, o, o_send.at[o], o_recv.at[o], {"kv": src}).start()

        return carry

    lax.fori_loop(0, N_KV, attend, 0)

    q_own = padded(q_all[0].astype(f32), 128)
    new = padded(kv_new[...], 128)
    k_own = new[:, :head_dim].astype(bf16)
    v_own = new[:, head_dim:].astype(bf16)
    seen = reach[...] > 0.5
    bias_tile = path_tile[...]
    new_parts, new_sums = [], []
    for h in range(heads):
        logits = dot_nt(q_own[:, h * head_dim : (h + 1) * head_dim].astype(bf16), k_own)
        logits = jnp.where(seen, logits - bias_tile[h : h + 1, :], floor_value)
        top = jnp.max(logits, axis=1, keepdims=True)
        weight = jnp.where(seen, jnp.exp(logits - top), 0.0)
        total_new = jnp.sum(weight, axis=1, keepdims=True)
        new_parts.append((dot(weight.astype(bf16), v_own) / total_new)[:share])
        new_sums.append(top + jnp.log(total_new))
    new_part = jnp.concatenate(new_parts, axis=1)
    columns = jnp.zeros((heads * drafts, 128), f32)
    for j in range(seqs):
        column = jnp.concatenate([s[j * drafts : (j + 1) * drafts] for s in new_sums], axis=0)
        columns = jnp.where(wide_lane == j, column, columns)
    new_tile = padded(columns, 128).T[:8]

    tiles = [l_send[0]]
    for o in range(1, N_KV):
        remote(LSE, o, l_send.at[o], l_recv.at[o], {"kv": ahead(o)}).wait_recv()
        tiles.append(l_recv[o])
    tiles.append(new_tile)
    top_all = functools.reduce(jnp.maximum, tiles)
    factors = [jnp.exp(t - top_all) for t in tiles]
    whole = functools.reduce(jnp.add, factors)
    shares = [f / whole for f in factors]
    spread = jnp.concatenate(shares[:N_KV], axis=0).T
    spread_new = jnp.concatenate([shares[N_KV]] * 16, axis=0).T
    low_half = lanes((drafts, 128)) < head_dim

    def factor_rows(table, at):
        parts = []
        for j in range(seqs):
            column = table[:, at + j : at + j + 1]
            parts.append(
                jnp.concatenate(
                    [
                        jnp.where(
                            low_half,
                            column[2 * g * drafts : (2 * g + 1) * drafts],
                            column[(2 * g + 1) * drafts : (2 * g + 2) * drafts],
                        )
                        for g in range(2)
                    ],
                    axis=1,
                )
            )
        return jnp.concatenate(parts, axis=0)

    merged = new_part * factor_rows(spread_new, 0) + o_send[0].astype(f32) * factor_rows(spread, 0)
    for o in range(1, N_KV):
        remote(PART, o, o_send.at[o], o_recv.at[o], {"kv": ahead(o)}).wait_recv()
        merged = merged + o_recv[o].astype(f32) * factor_rows(spread, 8 * o)
    a_all[0] = merged.astype(bf16)
    for o in range(1, N_KV):
        remote(ATT, o, a_all.at[0], a_all.at[o], {"kv": ahead(o)}).start()

    def place_of(o):
        chunk = behind(o)
        owner, half = chunk // 2, chunk % 2
        u = ((owner // 2 + 4 - x) % 4) * 2 + (owner % 2 + 2 - core) % 2
        return owner, half, u

    def out_copy(o):
        owner, half, u = place_of(o)
        return remote(OUT, u * 2 + half, t_send.at[o], t_recv.at[u * 2 + half], {"tp": owner})

    def output(o, carry):
        @pl.when(o > 0)
        def _():
            remote(ATT, o, a_all.at[0], a_all.at[o], {"kv": ahead(o)}).wait_recv()

        part = dot(a_all[o], w_out[...]).astype(bf16)
        owner, half, u = place_of(o)
        t_send[o] = part

        @pl.when(u == 0)
        def _():
            t_recv[half] = part

        @pl.when(u != 0)
        def _():
            out_copy(o).start()

        return carry

    lax.fori_loop(0, N_KV, output, 0)
    for half in range(2):
        summed = t_recv[half].astype(f32)
        for u in range(1, N_TP):
            at = u * 2 + half
            remote(OUT, at, t_send.at[0], t_recv.at[at], {"tp": tp_ahead(u)}).wait_recv()
            summed = summed + t_recv[at].astype(f32)
        fin[half] = summed.astype(bf16)
        out[tp * 2 + half] = summed.astype(bf16)
        for u in range(1, N_TP):
            remote(FINAL, u * 2 + half, fin.at[half], out.at[tp * 2 + half], {"tp": tp_ahead(u)}).start()
    for half in range(2):
        for u in range(1, N_TP):
            copy = remote(FINAL, u * 2 + half, fin.at[half], out.at[tp * 2 + half], {"tp": tp_ahead(u)})
            copy.wait_recv()
            copy.wait_send()
            remote(OUT, u * 2 + half, t_send.at[0], t_recv.at[u * 2 + half], {"tp": tp_ahead(u)}).wait_send()
    for o in range(1, N_KV):
        device = {"kv": ahead(o)}
        remote(STAT, o, s_send.at[o], s_recv.at[o], device).wait_send()
        remote(PROJ, o, p_send.at[o], p_recv.at[o], device).wait_send()
        remote(QUERY, o, q_all.at[0], q_all.at[o], device).wait_send()
        remote(LSE, o, l_send.at[o], l_recv.at[o], device).wait_send()
        remote(PART, o, o_send.at[o], o_recv.at[o], device).wait_send()
        remote(ATT, o, a_all.at[0], a_all.at[o], device).wait_send()


def body(
    tokens, norm_gain, w_query, w_key, w_value, w_forget, forget_bias, query_gain, key_gain, w_out,
    key_cache, value_cache, gate_sums, parents, lengths, accepted,
):
    seq_count, drafts, local_width = tokens.shape
    share = seq_count * drafts // N_KV
    vmem = pl.BlockSpec(memory_space=pltpu.VMEM)
    smem = pl.BlockSpec(memory_space=pltpu.SMEM)
    anywhere = pl.BlockSpec(memory_space=pl.ANY)
    mixed = pl.pallas_call(
        kernel,
        out_shape=jax.ShapeDtypeStruct((N_KV, share, local_width), bf16),
        in_specs=[
            vmem, vmem, vmem, vmem, vmem, anywhere, smem, vmem, vmem, vmem,
            anywhere, anywhere, anywhere, smem, smem, smem,
        ],
        out_specs=vmem,
        scratch_shapes=[
            pltpu.VMEM((local_width, 384), bf16),
            pltpu.VMEM((local_width, w_forget.shape[1]), bf16),
            pltpu.VMEM(key_cache.shape, bf16),
            pltpu.VMEM(value_cache.shape, bf16),
            pltpu.VMEM(gate_sums.shape, f32),
            pltpu.VMEM((128, 128), f32),
            pltpu.VMEM((N_KV, share, 384), bf16),
            pltpu.VMEM((N_KV, share, 384), bf16),
            pltpu.VMEM((N_KV, 8, 128), f32),
            pltpu.VMEM((N_KV, 8, 128), f32),
            pltpu.VMEM((share, 384), f32),
            pltpu.VMEM((N_KV, share, 256), bf16),
            pltpu.VMEM((share, 128), f32),
            pltpu.VMEM((8, 128), f32),
            pltpu.VMEM((N_KV, share, 256), bf16),
            pltpu.VMEM((N_KV, share, 256), bf16),
            pltpu.VMEM((N_KV, 8, 128), f32),
            pltpu.VMEM((N_KV, 8, 128), f32),
            pltpu.VMEM((N_KV, share, 256), bf16),
            pltpu.VMEM((N_KV, share, 256), bf16),
            pltpu.VMEM((N_KV, share, 256), bf16),
            pltpu.VMEM((2, share, 256), bf16),
            pltpu.SemaphoreType.DMA((4,)),
            pltpu.SemaphoreType.DMA((8, 16)),
            pltpu.SemaphoreType.DMA((8, 16)),
        ],
        compiler_params=pltpu.CompilerParams(
            collective_id=0, has_side_effects=True, vmem_limit_bytes=56 * 1024 * 1024
        ),
        name="tree_attention",
    )(
        tokens.reshape(N_KV, share, local_width), norm_gain.reshape(1, -1), w_query, w_key, w_value, w_forget,
        forget_bias, query_gain.reshape(1, -1), key_gain.reshape(1, -1), w_out,
        key_cache, value_cache, gate_sums, parents, lengths, accepted,
    )
    return mixed.reshape(seq_count, drafts, local_width)


def solution(mesh):
    return jax.shard_map(
        body,
        mesh=mesh,
        in_specs=(
            P(None, None, "kv"),
            P("kv"),
            P("kv", "tp"),
            P("kv", "tp"),
            P("kv", "tp"),
            P(),
            P("tp"),
            P(),
            P(),
            P("tp", "kv"),
            P(None, "tp", "kv"),
            P(None, "tp", "kv"),
            P(None, "tp", "kv"),
            P(),
            P(),
            P(),
        ),
        out_specs=P(None, None, "kv"),
        check_vma=False,
    )
```

```python
import functools

import jax
import jax.numpy as jnp
from jax import lax
from jax.experimental import pallas as pl
from jax.experimental.pallas import tpu as pltpu
from jax.sharding import PartitionSpec as P

f32, bf16 = jnp.float32, jnp.bfloat16
eps = 1e-05
floor_value = -1e30
KV_SIDE = 4
N_KV = 16
N_TP = 8
MESH = pl.DeviceIdType.MESH

PROJ, STAT, QUERY, PART, LSE, ATT, OUT, FINAL = range(8)


def dot(a, b):
    return jnp.dot(a, b, preferred_element_type=f32)


def dot_nt(a, b):
    return lax.dot_general(a, b, (((1,), (1,)), ((), ())), preferred_element_type=f32)


def halves(value):
    high = value.astype(bf16)
    return high, (value - high.astype(f32)).astype(bf16)


def padded(value, rows):
    return jnp.concatenate([value, jnp.zeros((rows - value.shape[0], value.shape[1]), value.dtype)], axis=0)


def lanes(shape):
    return lax.broadcasted_iota(jnp.int32, shape, 1)


def rows_of(shape):
    return lax.broadcasted_iota(jnp.int32, shape, 0)


def kernel(
    tokens, norm_gain, w_query, w_key, w_value, w_forget, forget_bias, query_gain, key_gain, w_out,
    key_cache, value_cache, gate_sums, parents, lengths, accepted,
    out,
    w_kv, wf, keys, values, gates, reach, p_send, p_recv, s_send, s_recv, own_proj, q_all, q_own, kv_own,
    new_out, new_tile, o_send, o_recv, l_send, l_recv, a_all, t_send, t_recv, fin,
    local_sem, send_sem, recv_sem,
):
    kv = lax.axis_index("kv")
    tp = lax.axis_index("tp")
    z, y = kv // KV_SIDE, kv % KV_SIDE
    x, core = tp // 2, tp % 2
    seqs = 3
    drafts = tokens.shape[1]
    share = seqs * drafts
    heads = 4
    head_dim = 64
    width = heads * head_dim
    positions = key_cache.shape[2]
    model_width = w_forget.shape[1]

    def ahead(o):
        return ((z + o // KV_SIDE) % KV_SIDE) * KV_SIDE + (y + o % KV_SIDE) % KV_SIDE

    def behind(o):
        return ((z + KV_SIDE - o // KV_SIDE) % KV_SIDE) * KV_SIDE + (y + KV_SIDE - o % KV_SIDE) % KV_SIDE

    def tp_ahead(u):
        return ((x + u // 2) % 4) * 2 + (core + u) % 2

    def remote(kind, j, src, dst, device):
        return pltpu.make_async_remote_copy(
            src_ref=src, dst_ref=dst, send_sem=send_sem.at[kind, j], recv_sem=recv_sem.at[kind, j],
            device_id=device, device_id_type=MESH,
        )

    def arrived(kind, j, ref):
        remote(kind, j, ref, ref, {"kv": ahead(1)}).wait_recv()

    def gone(kind, j, ref):
        remote(kind, j, ref, ref, {"kv": ahead(1)}).wait_send()

    def others(ref, j):
        return ref.at[pl.ds(j * N_KV + 1, N_KV - 1)]

    barrier = pltpu.get_barrier_semaphore()
    for o in range(1, N_KV):
        pl.semaphore_signal(barrier, inc=1, device_id={"kv": ahead(o)}, device_id_type=MESH)
    for u in range(1, N_TP):
        pl.semaphore_signal(barrier, inc=1, device_id={"tp": tp_ahead(u)}, device_id_type=MESH)

    wf_copy = pltpu.make_async_copy(w_forget.at[:, pl.ds(kv * 256, 256)], wf, local_sem.at[0])
    gate_copy = pltpu.make_async_copy(gate_sums, gates, local_sem.at[1])
    key_copy = pltpu.make_async_copy(key_cache, keys, local_sem.at[2])
    value_copy = pltpu.make_async_copy(value_cache, values.at[:, pl.ds(0, head_dim)], local_sem.at[3])
    wf_copy.start()
    gate_copy.start()
    key_copy.start()
    value_copy.start()

    w_kv[...] = jnp.concatenate([w_key[...].astype(f32), w_value[...].astype(f32)], axis=0).astype(bf16)
    wf_copy.wait()
    gate_copy.wait()
    pick = (lanes((8, 32)) == rows_of((8, 32)) + 4 * tp) & (rows_of((8, 32)) < 4)
    gate_weights = dot(pick.astype(f32).astype(bf16), wf[...]).astype(bf16)
    square_row = (rows_of((8, 256)) == 4).astype(f32).astype(bf16)
    gain = norm_gain[...].astype(f32)
    gain = jnp.concatenate([gain[0:1], gain[1:2]], axis=1)
    place = lanes((heads, positions)) + kv * positions
    tile_lane = lanes((8, 128))
    tile_row = rows_of((8, 128))

    def project(o, carry):
        chunk = ahead(o)
        wide = jnp.concatenate([tokens[chunk * seqs + j].astype(f32) for j in range(seqs)], axis=0)
        wide = padded(wide, 128)
        scaled = (wide * gain).astype(bf16)
        high, low = halves(wide * wide)
        tile = dot_nt(gate_weights, scaled) + dot_nt(square_row, high) + dot_nt(square_row, low)
        for j in range(seqs):
            b = chunk * seqs + j
            last = jnp.sum(
                jnp.where(place == lengths[b] + accepted[b] - 1, gates[b], 0.0), axis=1, keepdims=True
            )
            last = jnp.concatenate([last, jnp.zeros((4, 1), f32)], axis=0)
            tile = jnp.where(tile_lane == share + j, last, tile)
        s_send[o] = tile
        projected = jnp.concatenate([dot(scaled, w_query[...]), dot_nt(scaled, w_kv[...])], axis=1)
        for j in range(seqs):
            p_send[j * N_KV + o] = projected[j * drafts : (j + 1) * drafts].astype(bf16)
        own_proj[...] = projected[:share]
        return carry

    lax.fori_loop(0, N_KV, lambda i, c: project(N_KV - 1 - i, c), 0)

    pl.semaphore_wait(barrier, N_KV + N_TP - 2)
    for o in range(1, N_KV):
        remote(STAT, 0, s_send.at[o], s_recv.at[o], {"kv": ahead(o)}).start()
    for j in range(seqs):
        for o in range(1, N_KV):
            at = j * N_KV + o
            remote(PROJ, j, p_send.at[at], p_recv.at[at], {"kv": ahead(o)}).start()

    row_lane = lanes((1, 128))
    for j in range(seqs):
        for p in range(drafts):
            parent = parents[p, kv * seqs + j]
            at = jnp.where(parent >= 0, parent + drafts * j, -1)
            i = drafts * j + p
            reach[i : i + 1, :] = ((row_lane == i) | (row_lane == at)).astype(f32)
    reach[share:, :] = jnp.zeros((128 - share, 128), f32)
    closure = reach[...]
    for _ in range(5):
        closure = jnp.minimum(dot(closure.astype(bf16), closure.astype(bf16)), 1.0)
    reach[...] = closure

    def set_ones(b, carry):
        values[b, head_dim:, :] = jnp.ones((16, positions), bf16)
        return carry

    lax.fori_loop(0, values.shape[0], set_ones, 0)

    head_of = lax.broadcasted_iota(jnp.int32, (384, 384), 0) // head_dim
    head_at = lax.broadcasted_iota(jnp.int32, (384, 384), 1) // head_dim
    head_mean = jnp.where(head_of == head_at, 1.0 / head_dim, 0.0).astype(bf16)
    gains = jnp.concatenate([query_gain[...].astype(f32)] * 4 + [key_gain[...].astype(f32)] * 2, axis=1)
    q_own[share:, :] = jnp.zeros((128 - share, width), f32)
    kv_own[share:, :] = jnp.zeros((128 - share, 128), f32)

    arrived(STAT, 0, others(s_recv, 0))
    stats = s_send[0]
    for o in range(1, N_KV):
        stats = stats + s_recv[o]
    inverse_tile = lax.rsqrt(stats / model_width + eps)
    inverse = jnp.concatenate([inverse_tile] * 16, axis=0).T
    for j in range(seqs):
        rows = slice(j * drafts, (j + 1) * drafts)
        arrived(PROJ, j, others(p_recv, j))
        total = own_proj[rows, :]
        for o in range(1, N_KV):
            total = total + p_recv[j * N_KV + o].astype(f32)
        total = total * inverse[rows, 4:5]
        high, low = halves(total * total)
        mean_sq = dot(high, head_mean) + dot(low, head_mean)
        normed = total * lax.rsqrt(mean_sq + eps) * gains
        query = normed[:, :width].astype(bf16).astype(f32) * head_dim ** (-0.5)
        q_all[j * N_KV] = query.astype(bf16)
        for o in range(1, N_KV):
            remote(QUERY, j, q_all.at[j * N_KV], q_all.at[j * N_KV + o], {"kv": ahead(o)}).start()
        q_own[rows, :] = query
        kv_own[rows, :] = jnp.concatenate(
            [normed[:, width : width + head_dim], total[:, width + head_dim :]], axis=1
        )

    bias = jnp.where(
        tile_row == 0, forget_bias[0],
        jnp.where(tile_row == 1, forget_bias[1], jnp.where(tile_row == 2, forget_bias[2], forget_bias[3])),
    )
    gate_pre = stats * inverse_tile[4:5, :] + bias
    log_gate = jnp.minimum(gate_pre, 0.0) - jnp.log1p(jnp.exp(-jnp.abs(gate_pre)))
    log_gate = jnp.where(tile_lane < share, log_gate, 0.0)
    top_part = log_gate.astype(bf16)
    middle, last_part = halves(log_gate - top_part.astype(f32))
    follows = reach[...].astype(bf16)
    path = dot_nt(top_part, follows) + dot_nt(middle, follows) + dot_nt(last_part, follows)
    last_gate = jnp.where(
        tile_lane < drafts, stats[:, share : share + 1],
        jnp.where(tile_lane < 2 * drafts, stats[:, share + 1 : share + 2], stats[:, share + 2 : share + 3]),
    )
    bias_tile = path + last_gate

    wide_lane = lanes((heads * drafts, 128))
    own_queries = q_own[...]
    k_own = kv_own[:, :head_dim].astype(bf16)
    v_own = kv_own[:, head_dim:].astype(bf16)
    seen = reach[...] > 0.5
    new_parts, new_sums = [], []
    for h in range(heads):
        logits = dot_nt(own_queries[:, h * head_dim : (h + 1) * head_dim].astype(bf16), k_own)
        logits = jnp.where(seen, logits - bias_tile[h : h + 1, :], floor_value)
        top = jnp.max(logits, axis=1, keepdims=True)
        weight = jnp.where(seen, jnp.exp(logits - top), 0.0)
        total_new = jnp.sum(weight, axis=1, keepdims=True)
        new_parts.append((dot(weight.astype(bf16), v_own) / total_new)[:share])
        new_sums.append(top + jnp.log(total_new))
    new_out[...] = jnp.concatenate(new_parts, axis=1)
    columns = jnp.zeros((heads * drafts, 128), f32)
    for j in range(seqs):
        column = jnp.concatenate([s[j * drafts : (j + 1) * drafts] for s in new_sums], axis=0)
        columns = jnp.where(wide_lane == j, column, columns)
    new_tile[...] = padded(columns, 128).T[:8]

    key_copy.wait()
    value_copy.wait()

    def attend(j, o, sums):
        src = behind(o)
        b = src * seqs + j
        at = j * N_KV + o
        block = q_all[at].astype(f32)
        stacked = jnp.concatenate(
            [block[:, h * head_dim : (h + 1) * head_dim] for h in range(heads)], axis=0
        ).astype(bf16)
        logits = dot(stacked, keys[b])
        kept = jnp.where(place < lengths[b] + accepted[b], -gates[b], floor_value)
        tops, weights = [], []
        for h in range(heads):
            row = logits[h * drafts : (h + 1) * drafts] + kept[h : h + 1]
            top = jnp.max(row, axis=1, keepdims=True)
            tops.append(top)
            weights.append(jnp.exp(row - top))
        weighted = dot_nt(jnp.concatenate(weights, axis=0).astype(bf16), values[b])
        total = weighted[:, head_dim : head_dim + 1]
        weighted = weighted[:, :head_dim] / total
        o_send[at] = jnp.concatenate(
            [weighted[h * drafts : (h + 1) * drafts] for h in range(heads)], axis=1
        ).astype(bf16)
        if o > 0:
            remote(PART, j, o_send.at[at], o_recv.at[at], {"kv": src}).start()
        return jnp.where(wide_lane == o, jnp.concatenate(tops, axis=0) + jnp.log(total), sums)

    def attend_all(j, first, last, sums):
        for o in range(first, last):
            if o == 1:
                arrived(QUERY, j, others(q_all, j))
            sums = attend(j, o, sums)
        if last < N_KV:
            return sums
        table = padded(sums, 128).T
        l_recv[j * N_KV] = table[:1]
        for o in range(1, N_KV):
            at = j * N_KV + o
            l_send[at] = table[o : o + 1]
        for o in range(1, N_KV):
            at = j * N_KV + o
            remote(LSE, j, l_send.at[at], l_recv.at[at], {"kv": behind(o)}).start()
        return sums

    low_half = lanes((drafts, 128)) < head_dim

    def merge(j):
        arrived(LSE, j, others(l_recv, j))
        table = jnp.concatenate([l_recv[j * N_KV + o] for o in range(N_KV)], axis=0)
        new = new_tile[j : j + 1, :]
        top = jnp.maximum(jnp.max(table, axis=0, keepdims=True), new)
        factors = jnp.exp(table - top)
        factor_new = jnp.exp(new - top)
        whole = jnp.sum(factors, axis=0, keepdims=True) + factor_new
        spread = padded(jnp.concatenate([factors / whole, padded(factor_new / whole, 8)], axis=0), 128).T

        def factor_rows(at):
            column = spread[:, at : at + 1]
            return jnp.concatenate(
                [
                    jnp.where(
                        low_half,
                        column[2 * g * drafts : (2 * g + 1) * drafts],
                        column[(2 * g + 1) * drafts : (2 * g + 2) * drafts],
                    )
                    for g in range(2)
                ],
                axis=1,
            )

        merged = new_out[j * drafts : (j + 1) * drafts, :] * factor_rows(N_KV)
        merged = merged + o_send[j * N_KV].astype(f32) * factor_rows(0)
        arrived(PART, j, others(o_recv, j))
        for o in range(1, N_KV):
            merged = merged + o_recv[j * N_KV + o].astype(f32) * factor_rows(o)
        a_all[j * N_KV] = merged.astype(bf16)
        for o in range(1, N_KV):
            remote(ATT, j, a_all.at[j * N_KV], a_all.at[j * N_KV + o], {"kv": ahead(o)}).start()

    def output(j):
        arrived(ATT, j, others(a_all, j))
        rows = jnp.concatenate([a_all[j * N_KV + o].astype(f32) for o in range(N_KV)], axis=0).astype(bf16)
        part = dot(rows, w_out[...])
        for o in range(N_KV):
            t_send[j * N_KV + o] = part[o * drafts : (o + 1) * drafts].astype(bf16)
        for u in range(N_TP):
            owner = tp_ahead(u)
            for half in range(2):
                chunk = owner * 2 + half
                o = ((z + 4 - chunk // 4) % 4) * 4 + (y + 4 - chunk % 4) % 4
                at = j * N_KV + u * 2 + half
                if u == 0:
                    t_recv[at] = t_send[j * N_KV + o]
                else:
                    remote(OUT, j, t_send.at[j * N_KV + o], t_recv.at[at], {"tp": owner}).start()

    def add_up(j):
        arrived(OUT, j, t_recv.at[pl.ds(j * N_KV + 2, N_KV - 2)])
        for half in range(2):
            summed = t_recv[j * N_KV + half].astype(f32)
            for u in range(1, N_TP):
                summed = summed + t_recv[j * N_KV + u * 2 + half].astype(f32)
            seq = (tp * 2 + half) * seqs + j
            fin[j * 2 + half] = summed.astype(bf16)
            out[seq] = summed.astype(bf16)
            for u in range(1, N_TP):
                remote(FINAL, j, fin.at[j * 2 + half], out.at[seq], {"tp": tp_ahead(u)}).start()

    none = jnp.zeros((heads * drafts, 128), f32)
    attend_all(0, 0, N_KV, none)
    attend_all(1, 0, N_KV, none)
    merge(0)
    sums = attend_all(2, 0, 10, none)
    merge(1)
    attend_all(2, 10, N_KV, sums)
    output(0)
    merge(2)
    output(1)
    add_up(0)
    add_up(1)
    output(2)
    add_up(2)
    for j in range(seqs):
        arrived(FINAL, j, t_recv.at[pl.ds(j * N_KV + 2, N_KV - 2)])
    gone(STAT, 0, others(s_send, 0))
    for j in range(seqs):
        gone(PROJ, j, others(p_send, j))
        gone(QUERY, j, others(q_all, j))
        gone(PART, j, others(o_send, j))
        gone(LSE, j, others(l_send, j))
        gone(ATT, j, others(a_all, j))
        gone(OUT, j, t_send.at[pl.ds(j * N_KV + 2, N_KV - 2)])
        gone(FINAL, j, t_send.at[pl.ds(j * N_KV + 2, N_KV - 2)])


def body(
    tokens, norm_gain, w_query, w_key, w_value, w_forget, forget_bias, query_gain, key_gain, w_out,
    key_cache, value_cache, gate_sums, parents, lengths, accepted,
):
    seq_count, drafts, local_width = tokens.shape
    share = seq_count * drafts // N_KV
    vmem = pl.BlockSpec(memory_space=pltpu.VMEM)
    smem = pl.BlockSpec(memory_space=pltpu.SMEM)
    anywhere = pl.BlockSpec(memory_space=pl.ANY)
    mixed = pl.pallas_call(
        kernel,
        out_shape=jax.ShapeDtypeStruct(tokens.shape, bf16),
        in_specs=[
            vmem, vmem, vmem, vmem, vmem, anywhere, smem, vmem, vmem, vmem,
            anywhere, anywhere, anywhere, smem, smem, smem,
        ],
        out_specs=vmem,
        scratch_shapes=[
            pltpu.VMEM((128, local_width), bf16),
            pltpu.VMEM((w_forget.shape[1], local_width), bf16),
            pltpu.VMEM(key_cache.shape, bf16),
            pltpu.VMEM((seq_count, value_cache.shape[1] + 16, value_cache.shape[2]), bf16),
            pltpu.VMEM(gate_sums.shape, f32),
            pltpu.VMEM((128, 128), f32),
            pltpu.VMEM((seq_count, drafts, 384), bf16),
            pltpu.VMEM((seq_count, drafts, 384), bf16),
            pltpu.VMEM((N_KV, 8, 128), f32),
            pltpu.VMEM((N_KV, 8, 128), f32),
            pltpu.VMEM((share, 384), f32),
            pltpu.VMEM((seq_count, drafts, 256), bf16),
            pltpu.VMEM((128, 256), f32),
            pltpu.VMEM((128, 128), f32),
            pltpu.VMEM((share, 256), f32),
            pltpu.VMEM((8, 128), f32),
            pltpu.VMEM((seq_count, drafts, 256), bf16),
            pltpu.VMEM((seq_count, drafts, 256), bf16),
            pltpu.VMEM((seq_count, 1, 128), f32),
            pltpu.VMEM((seq_count, 1, 128), f32),
            pltpu.VMEM((seq_count, drafts, 256), bf16),
            pltpu.VMEM((seq_count, drafts, 256), bf16),
            pltpu.VMEM((seq_count, drafts, 256), bf16),
            pltpu.VMEM((6, drafts, 256), bf16),
            pltpu.SemaphoreType.DMA((4,)),
            pltpu.SemaphoreType.DMA((8, 3)),
            pltpu.SemaphoreType.DMA((8, 3)),
        ],
        compiler_params=pltpu.CompilerParams(
            collective_id=0, has_side_effects=True, vmem_limit_bytes=56 * 1024 * 1024
        ),
        name="tree_attention",
    )(
        tokens, norm_gain.reshape(2, -1), w_query, w_key.T, w_value.T, w_forget.T,
        forget_bias, query_gain.reshape(1, -1), key_gain.reshape(1, -1), w_out,
        key_cache, value_cache, gate_sums, parents.T, lengths, accepted,
    )
    return mixed


def solution(mesh):
    return jax.shard_map(
        body,
        mesh=mesh,
        in_specs=(
            P(None, None, "kv"),
            P("kv"),
            P("kv", "tp"),
            P("kv", "tp"),
            P("kv", "tp"),
            P(),
            P("tp"),
            P(),
            P(),
            P("tp", "kv"),
            P(None, "tp", "kv"),
            P(None, "tp", "kv"),
            P(None, "tp", "kv"),
            P(),
            P(),
            P(),
        ),
        out_specs=P(None, None, "kv"),
        check_vma=False,
    )
```

```python
import functools

import jax
import jax.numpy as jnp
from jax import lax
from jax.experimental import pallas as pl
from jax.experimental.pallas import tpu as pltpu
from jax.sharding import PartitionSpec as P

f32, bf16 = jnp.float32, jnp.bfloat16
eps = 1e-05
floor_value = -1e30
KV_SIDE = 4
N_KV = 16
N_TP = 8
GROUPS = ((0, 1), (1, 6), (6, 11), (11, 16))
MESH = pl.DeviceIdType.MESH

PROJ, STAT, QUERY, PART, LSE, ATT, OUT, FINAL = range(8)


def dot(a, b):
    return jnp.dot(a, b, preferred_element_type=f32)


def dot_nt(a, b):
    return lax.dot_general(a, b, (((1,), (1,)), ((), ())), preferred_element_type=f32)


def halves(value):
    high = value.astype(bf16)
    return high, (value - high.astype(f32)).astype(bf16)


def padded(value, rows):
    return jnp.concatenate([value, jnp.zeros((rows - value.shape[0], value.shape[1]), value.dtype)], axis=0)


def lanes(shape):
    return lax.broadcasted_iota(jnp.int32, shape, 1)


def rows_of(shape):
    return lax.broadcasted_iota(jnp.int32, shape, 0)


def kernel(
    tokens, norm_gain, w_query, w_key, w_value, w_forget, forget_bias, query_gain, key_gain, w_out,
    key_cache, value_cache, gate_sums, parents, lengths, accepted,
    out,
    w_kv, wf, keys, values, gates, reach, p_send, p_recv, s_send, s_recv, own_proj, q_all, q_own, kv_own,
    new_out, new_tile, o_send, o_recv, l_send, l_recv, a_all, t_send, t_recv, fin,
    local_sem, send_sem, recv_sem,
):
    kv = lax.axis_index("kv")
    tp = lax.axis_index("tp")
    z, y = kv // KV_SIDE, kv % KV_SIDE
    x, core = tp // 2, tp % 2
    seqs = 3
    drafts = tokens.shape[1]
    share = seqs * drafts
    heads = 4
    head_dim = 64
    width = heads * head_dim
    positions = key_cache.shape[2]
    model_width = w_forget.shape[1]

    def ahead(o):
        return ((z + o // KV_SIDE) % KV_SIDE) * KV_SIDE + (y + o % KV_SIDE) % KV_SIDE

    def behind(o):
        return ((z + KV_SIDE - o // KV_SIDE) % KV_SIDE) * KV_SIDE + (y + KV_SIDE - o % KV_SIDE) % KV_SIDE

    def tp_ahead(u):
        return ((x + u // 2) % 4) * 2 + (core + u) % 2

    def remote(kind, j, src, dst, device):
        return pltpu.make_async_remote_copy(
            src_ref=src, dst_ref=dst, send_sem=send_sem.at[kind, j], recv_sem=recv_sem.at[kind, j],
            device_id=device, device_id_type=MESH,
        )

    def arrived(kind, j, ref):
        remote(kind, j, ref, ref, {"kv": ahead(1)}).wait_recv()

    def gone(kind, j, ref):
        remote(kind, j, ref, ref, {"kv": ahead(1)}).wait_send()

    def others(ref, j):
        return ref.at[pl.ds(j * N_KV + 1, N_KV - 1)]

    barrier = pltpu.get_barrier_semaphore()
    for o in range(1, N_KV):
        pl.semaphore_signal(barrier, inc=1, device_id={"kv": ahead(o)}, device_id_type=MESH)
    for u in range(1, N_TP):
        pl.semaphore_signal(barrier, inc=1, device_id={"tp": tp_ahead(u)}, device_id_type=MESH)

    wf_copy = pltpu.make_async_copy(w_forget.at[:, pl.ds(kv * 256, 256)], wf, local_sem.at[0])
    gate_copy = pltpu.make_async_copy(gate_sums, gates, local_sem.at[1])
    key_copy = pltpu.make_async_copy(key_cache, keys, local_sem.at[2])
    value_copy = pltpu.make_async_copy(value_cache, values.at[:, pl.ds(0, head_dim)], local_sem.at[3])
    wf_copy.start()
    gate_copy.start()
    key_copy.start()
    value_copy.start()

    w_kv[...] = jnp.concatenate([w_key[...].astype(f32), w_value[...].astype(f32)], axis=0).astype(bf16)
    wf_copy.wait()
    gate_copy.wait()
    pick = (lanes((8, 32)) == rows_of((8, 32)) + 4 * tp) & (rows_of((8, 32)) < 4)
    gate_weights = dot(pick.astype(f32).astype(bf16), wf[...]).astype(bf16)
    square_row = (rows_of((8, 256)) == 4).astype(f32).astype(bf16)
    gain = norm_gain[...].astype(f32)
    gain = jnp.concatenate([gain[0:1], gain[1:2]], axis=1)
    place = lanes((heads, positions)) + kv * positions
    tile_lane = lanes((8, 128))
    tile_row = rows_of((8, 128))

    def project(o, carry):
        chunk = ahead(o)
        wide = jnp.concatenate([tokens[chunk * seqs + j].astype(f32) for j in range(seqs)], axis=0)
        wide = padded(wide, 128)
        scaled = (wide * gain).astype(bf16)
        high, low = halves(wide * wide)
        tile = dot_nt(gate_weights, scaled) + dot_nt(square_row, high) + dot_nt(square_row, low)
        for j in range(seqs):
            b = chunk * seqs + j
            last = jnp.sum(
                jnp.where(place == lengths[b] + accepted[b] - 1, gates[b], 0.0), axis=1, keepdims=True
            )
            last = jnp.concatenate([last, jnp.zeros((4, 1), f32)], axis=0)
            tile = jnp.where(tile_lane == share + j, last, tile)
        s_send[o] = tile
        projected = jnp.concatenate([dot(scaled, w_query[...]), dot_nt(scaled, w_kv[...])], axis=1)
        for j in range(seqs):
            p_send[j * N_KV + o] = projected[j * drafts : (j + 1) * drafts].astype(bf16)
        own_proj[...] = projected[:share]
        return carry

    def project_four(i, carry):
        for k in range(4):
            project(N_KV - 1 - 4 * i - k, carry)
        return carry

    lax.fori_loop(0, N_KV // 4, project_four, 0)

    pl.semaphore_wait(barrier, N_KV + N_TP - 2)
    for o in range(1, N_KV):
        remote(STAT, 0, s_send.at[o], s_recv.at[o], {"kv": ahead(o)}).start()
    for j in range(seqs):
        for o in range(1, N_KV):
            at = j * N_KV + o
            remote(PROJ, j, p_send.at[at], p_recv.at[at], {"kv": ahead(o)}).start()

    row_lane = lanes((1, 128))
    for j in range(seqs):
        for p in range(drafts):
            parent = parents[p, kv * seqs + j]
            at = jnp.where(parent >= 0, parent + drafts * j, -1)
            i = drafts * j + p
            reach[i : i + 1, :] = ((row_lane == i) | (row_lane == at)).astype(f32)
    reach[share:, :] = jnp.zeros((128 - share, 128), f32)
    closure = reach[...]
    for _ in range(5):
        closure = jnp.minimum(dot(closure.astype(bf16), closure.astype(bf16)), 1.0)
    reach[...] = closure

    def set_ones(b, carry):
        values[b, head_dim:, :] = jnp.ones((16, positions), bf16)
        return carry

    lax.fori_loop(0, values.shape[0], set_ones, 0)

    head_of = lax.broadcasted_iota(jnp.int32, (384, 384), 0) // head_dim
    head_at = lax.broadcasted_iota(jnp.int32, (384, 384), 1) // head_dim
    head_mean = jnp.where(head_of == head_at, 1.0 / head_dim, 0.0).astype(bf16)
    gains = jnp.concatenate([query_gain[...].astype(f32)] * 4 + [key_gain[...].astype(f32)] * 2, axis=1)
    q_own[share:, :] = jnp.zeros((128 - share, width), f32)
    kv_own[share:, :] = jnp.zeros((128 - share, 128), f32)

    arrived(STAT, 0, others(s_recv, 0))
    stats = s_send[0]
    for o in range(1, N_KV):
        stats = stats + s_recv[o]
    inverse_tile = lax.rsqrt(stats / model_width + eps)
    inverse = jnp.concatenate([inverse_tile] * 16, axis=0).T
    for j in range(seqs):
        rows = slice(j * drafts, (j + 1) * drafts)
        arrived(PROJ, j, others(p_recv, j))
        total = own_proj[rows, :]
        for o in range(1, N_KV):
            total = total + p_recv[j * N_KV + o].astype(f32)
        total = total * inverse[rows, 4:5]
        high, low = halves(total * total)
        mean_sq = dot(high, head_mean) + dot(low, head_mean)
        normed = total * lax.rsqrt(mean_sq + eps) * gains
        query = normed[:, :width].astype(bf16).astype(f32) * head_dim ** (-0.5)
        q_all[j * N_KV] = query.astype(bf16)
        for o in range(1, N_KV):
            remote(QUERY, j, q_all.at[j * N_KV], q_all.at[j * N_KV + o], {"kv": ahead(o)}).start()
        q_own[rows, :] = query
        kv_own[rows, :] = jnp.concatenate(
            [normed[:, width : width + head_dim], total[:, width + head_dim :]], axis=1
        )

    bias = jnp.where(
        tile_row == 0, forget_bias[0],
        jnp.where(tile_row == 1, forget_bias[1], jnp.where(tile_row == 2, forget_bias[2], forget_bias[3])),
    )
    gate_pre = stats * inverse_tile[4:5, :] + bias
    log_gate = jnp.minimum(gate_pre, 0.0) - jnp.log1p(jnp.exp(-jnp.abs(gate_pre)))
    log_gate = jnp.where(tile_lane < share, log_gate, 0.0)
    top_part = log_gate.astype(bf16)
    middle, last_part = halves(log_gate - top_part.astype(f32))
    follows = reach[...].astype(bf16)
    path = dot_nt(top_part, follows) + dot_nt(middle, follows) + dot_nt(last_part, follows)
    last_gate = jnp.where(
        tile_lane < drafts, stats[:, share : share + 1],
        jnp.where(tile_lane < 2 * drafts, stats[:, share + 1 : share + 2], stats[:, share + 2 : share + 3]),
    )
    bias_tile = path + last_gate

    wide_lane = lanes((heads * drafts, 128))
    own_queries = q_own[...]
    k_own = kv_own[:, :head_dim].astype(bf16)
    v_own = kv_own[:, head_dim:].astype(bf16)
    seen = reach[...] > 0.5
    new_parts, new_sums = [], []
    for h in range(heads):
        logits = dot_nt(own_queries[:, h * head_dim : (h + 1) * head_dim].astype(bf16), k_own)
        logits = jnp.where(seen, logits - bias_tile[h : h + 1, :], floor_value)
        top = jnp.max(logits, axis=1, keepdims=True)
        weight = jnp.where(seen, jnp.exp(logits - top), 0.0)
        total_new = jnp.sum(weight, axis=1, keepdims=True)
        new_parts.append((dot(weight.astype(bf16), v_own) / total_new)[:share])
        new_sums.append(top + jnp.log(total_new))
    new_out[...] = jnp.concatenate(new_parts, axis=1)
    columns = jnp.zeros((heads * drafts, 128), f32)
    for j in range(seqs):
        column = jnp.concatenate([s[j * drafts : (j + 1) * drafts] for s in new_sums], axis=0)
        columns = jnp.where(wide_lane == j, column, columns)
    new_tile[...] = padded(columns, 128).T[:8]

    key_copy.wait()
    value_copy.wait()

    def attend(j, o, sums):
        src = behind(o)
        b = src * seqs + j
        at = j * N_KV + o
        block = q_all[at].astype(f32)
        stacked = jnp.concatenate(
            [block[:, h * head_dim : (h + 1) * head_dim] for h in range(heads)], axis=0
        ).astype(bf16)
        logits = dot(stacked, keys[b])
        kept = jnp.where(place < lengths[b] + accepted[b], -gates[b], floor_value)
        tops, weights = [], []
        for h in range(heads):
            row = logits[h * drafts : (h + 1) * drafts] + kept[h : h + 1]
            top = jnp.max(row, axis=1, keepdims=True)
            tops.append(top)
            weights.append(jnp.exp(row - top))
        weighted = dot_nt(jnp.concatenate(weights, axis=0).astype(bf16), values[b])
        total = weighted[:, head_dim : head_dim + 1]
        weighted = weighted[:, :head_dim] / total
        o_send[at] = jnp.concatenate(
            [weighted[h * drafts : (h + 1) * drafts] for h in range(heads)], axis=1
        ).astype(bf16)
        return jnp.where(wide_lane == o, jnp.concatenate(tops, axis=0) + jnp.log(total), sums)

    def attend_all(j, first, last, sums):
        for start, stop in GROUPS:
            if start < first or stop > last:
                continue
            if start == 1:
                arrived(QUERY, j, others(q_all, j))
            for o in range(start, stop):
                sums = attend(j, o, sums)
            for o in range(max(start, 1), stop):
                at = j * N_KV + o
                remote(PART, j, o_send.at[at], o_recv.at[at], {"kv": behind(o)}).start()
        if last < N_KV:
            return sums
        table = padded(sums, 128).T
        l_recv[j * N_KV] = table[:1]
        for o in range(1, N_KV):
            at = j * N_KV + o
            l_send[at] = table[o : o + 1]
        for o in range(1, N_KV):
            at = j * N_KV + o
            remote(LSE, j, l_send.at[at], l_recv.at[at], {"kv": behind(o)}).start()
        return sums

    low_half = lanes((drafts, 128)) < head_dim

    def merge(j):
        arrived(LSE, j, others(l_recv, j))
        table = jnp.concatenate([l_recv[j * N_KV + o] for o in range(N_KV)], axis=0)
        new = new_tile[j : j + 1, :]
        top = jnp.maximum(jnp.max(table, axis=0, keepdims=True), new)
        factors = jnp.exp(table - top)
        factor_new = jnp.exp(new - top)
        whole = jnp.sum(factors, axis=0, keepdims=True) + factor_new
        spread = padded(jnp.concatenate([factors / whole, padded(factor_new / whole, 8)], axis=0), 128).T

        def factor_rows(at):
            column = spread[:, at : at + 1]
            return jnp.concatenate(
                [
                    jnp.where(
                        low_half,
                        column[2 * g * drafts : (2 * g + 1) * drafts],
                        column[(2 * g + 1) * drafts : (2 * g + 2) * drafts],
                    )
                    for g in range(2)
                ],
                axis=1,
            )

        merged = new_out[j * drafts : (j + 1) * drafts, :] * factor_rows(N_KV)
        merged = merged + o_send[j * N_KV].astype(f32) * factor_rows(0)
        arrived(PART, j, others(o_recv, j))
        for o in range(1, N_KV):
            merged = merged + o_recv[j * N_KV + o].astype(f32) * factor_rows(o)
        a_all[j * N_KV] = merged.astype(bf16)
        for o in range(1, N_KV):
            remote(ATT, j, a_all.at[j * N_KV], a_all.at[j * N_KV + o], {"kv": ahead(o)}).start()

    def output(j):
        arrived(ATT, j, others(a_all, j))
        rows = jnp.concatenate([a_all[j * N_KV + o].astype(f32) for o in range(N_KV)], axis=0).astype(bf16)
        part = dot(rows, w_out[...])
        for o in range(N_KV):
            t_send[j * N_KV + o] = part[o * drafts : (o + 1) * drafts].astype(bf16)
        for u in range(N_TP):
            owner = tp_ahead(u)
            for half in range(2):
                chunk = owner * 2 + half
                o = ((z + 4 - chunk // 4) % 4) * 4 + (y + 4 - chunk % 4) % 4
                at = j * N_KV + u * 2 + half
                if u == 0:
                    t_recv[at] = t_send[j * N_KV + o]
                else:
                    remote(OUT, j, t_send.at[j * N_KV + o], t_recv.at[at], {"tp": owner}).start()

    def add_up(j):
        arrived(OUT, j, t_recv.at[pl.ds(j * N_KV + 2, N_KV - 2)])
        for half in range(2):
            summed = t_recv[j * N_KV + half].astype(f32)
            for u in range(1, N_TP):
                summed = summed + t_recv[j * N_KV + u * 2 + half].astype(f32)
            seq = (tp * 2 + half) * seqs + j
            fin[j * 2 + half] = summed.astype(bf16)
            for u in range(1, N_TP):
                remote(FINAL, j, fin.at[j * 2 + half], out.at[seq], {"tp": tp_ahead(u)}).start()
            pltpu.make_async_copy(fin.at[j * 2 + half], out.at[seq], local_sem.at[4 + j * 2 + half]).start()

    none = jnp.zeros((heads * drafts, 128), f32)
    attend_all(0, 0, N_KV, none)
    attend_all(1, 0, N_KV, none)
    merge(0)
    sums = attend_all(2, 0, 11, none)
    merge(1)
    attend_all(2, 11, N_KV, sums)
    output(0)
    merge(2)
    output(1)
    add_up(0)
    add_up(1)
    output(2)
    add_up(2)
    for j in range(seqs):
        arrived(FINAL, j, t_recv.at[pl.ds(j * N_KV + 2, N_KV - 2)])
        for half in range(2):
            seq = (tp * 2 + half) * seqs + j
            pltpu.make_async_copy(fin.at[j * 2 + half], out.at[seq], local_sem.at[4 + j * 2 + half]).wait()
    gone(STAT, 0, others(s_send, 0))
    for j in range(seqs):
        gone(PROJ, j, others(p_send, j))
        gone(QUERY, j, others(q_all, j))
        gone(PART, j, others(o_send, j))
        gone(LSE, j, others(l_send, j))
        gone(ATT, j, others(a_all, j))
        gone(OUT, j, t_send.at[pl.ds(j * N_KV + 2, N_KV - 2)])
        gone(FINAL, j, t_send.at[pl.ds(j * N_KV + 2, N_KV - 2)])


def body(
    tokens, norm_gain, w_query, w_key, w_value, w_forget, forget_bias, query_gain, key_gain, w_out,
    key_cache, value_cache, gate_sums, parents, lengths, accepted,
):
    seq_count, drafts, local_width = tokens.shape
    share = seq_count * drafts // N_KV
    vmem = pl.BlockSpec(memory_space=pltpu.VMEM)
    smem = pl.BlockSpec(memory_space=pltpu.SMEM)
    anywhere = pl.BlockSpec(memory_space=pl.ANY)
    mixed = pl.pallas_call(
        kernel,
        out_shape=jax.ShapeDtypeStruct(tokens.shape, bf16),
        in_specs=[
            vmem, vmem, vmem, vmem, vmem, anywhere, smem, vmem, vmem, vmem,
            anywhere, anywhere, anywhere, smem, smem, smem,
        ],
        out_specs=anywhere,
        scratch_shapes=[
            pltpu.VMEM((128, local_width), bf16),
            pltpu.VMEM((w_forget.shape[1], local_width), bf16),
            pltpu.VMEM(key_cache.shape, bf16),
            pltpu.VMEM((seq_count, value_cache.shape[1] + 16, value_cache.shape[2]), bf16),
            pltpu.VMEM(gate_sums.shape, f32),
            pltpu.VMEM((128, 128), f32),
            pltpu.VMEM((seq_count, drafts, 384), bf16),
            pltpu.VMEM((seq_count, drafts, 384), bf16),
            pltpu.VMEM((N_KV, 8, 128), f32),
            pltpu.VMEM((N_KV, 8, 128), f32),
            pltpu.VMEM((share, 384), f32),
            pltpu.VMEM((seq_count, drafts, 256), bf16),
            pltpu.VMEM((128, 256), f32),
            pltpu.VMEM((128, 128), f32),
            pltpu.VMEM((share, 256), f32),
            pltpu.VMEM((8, 128), f32),
            pltpu.VMEM((seq_count, drafts, 256), bf16),
            pltpu.VMEM((seq_count, drafts, 256), bf16),
            pltpu.VMEM((seq_count, 1, 128), f32),
            pltpu.VMEM((seq_count, 1, 128), f32),
            pltpu.VMEM((seq_count, drafts, 256), bf16),
            pltpu.VMEM((seq_count, drafts, 256), bf16),
            pltpu.VMEM((seq_count, drafts, 256), bf16),
            pltpu.VMEM((6, drafts, 256), bf16),
            pltpu.SemaphoreType.DMA((10,)),
            pltpu.SemaphoreType.DMA((8, 3)),
            pltpu.SemaphoreType.DMA((8, 3)),
        ],
        compiler_params=pltpu.CompilerParams(
            collective_id=0, has_side_effects=True, vmem_limit_bytes=56 * 1024 * 1024
        ),
        name="tree_attention",
    )(
        tokens, norm_gain.reshape(2, -1), w_query, w_key.T, w_value.T, w_forget.T,
        forget_bias, query_gain.reshape(1, -1), key_gain.reshape(1, -1), w_out,
        key_cache, value_cache, gate_sums, parents.T, lengths, accepted,
    )
    return mixed


def solution(mesh):
    return jax.shard_map(
        body,
        mesh=mesh,
        in_specs=(
            P(None, None, "kv"),
            P("kv"),
            P("kv", "tp"),
            P("kv", "tp"),
            P("kv", "tp"),
            P(),
            P("tp"),
            P(),
            P(),
            P("tp", "kv"),
            P(None, "tp", "kv"),
            P(None, "tp", "kv"),
            P(None, "tp", "kv"),
            P(),
            P(),
            P(),
        ),
        out_specs=P(None, None, "kv"),
        check_vma=False,
    )
```

```python
import functools

import jax
import jax.numpy as jnp
from jax import lax
from jax.experimental import pallas as pl
from jax.experimental.pallas import tpu as pltpu
from jax.sharding import PartitionSpec as P

f32, bf16 = jnp.float32, jnp.bfloat16
eps = 1e-05
floor_value = -1e30
KV_SIDE = 4
N_KV = 16
N_TP = 8
GROUPS = ((0, 1), (1, 6), (6, 11), (11, 16))
MESH = pl.DeviceIdType.MESH

PROJ, STAT, QUERY, PART, LSE, ATT, OUT, FINAL = range(8)


def dot(a, b):
    return jnp.dot(a, b, preferred_element_type=f32)


def dot_nt(a, b):
    return lax.dot_general(a, b, (((1,), (1,)), ((), ())), preferred_element_type=f32)


def halves(value):
    high = value.astype(bf16)
    return high, (value - high.astype(f32)).astype(bf16)


def padded(value, rows):
    return jnp.concatenate([value, jnp.zeros((rows - value.shape[0], value.shape[1]), value.dtype)], axis=0)


def lanes(shape):
    return lax.broadcasted_iota(jnp.int32, shape, 1)


def rows_of(shape):
    return lax.broadcasted_iota(jnp.int32, shape, 0)


def kernel(
    tokens, norm_gain, w_query, w_key, w_value, w_forget, forget_bias, query_gain, key_gain, w_out,
    key_cache, value_cache, gate_sums, parents, lengths, accepted,
    out,
    w_kv, wf, keys, values, gates, reach, p_send, p_recv, s_send, s_recv, own_proj, q_all, q_own, kv_own,
    new_out, new_tile, o_send, o_recv, l_send, l_recv, a_all, t_send, t_recv, fin,
    local_sem, send_sem, recv_sem,
):
    kv = lax.axis_index("kv")
    tp = lax.axis_index("tp")
    z, y = kv // KV_SIDE, kv % KV_SIDE
    x, core = tp // 2, tp % 2
    seqs = 3
    drafts = tokens.shape[1]
    share = seqs * drafts
    heads = 4
    head_dim = 64
    width = heads * head_dim
    positions = key_cache.shape[2]
    model_width = w_forget.shape[1]

    def ahead(o):
        return ((z + o // KV_SIDE) % KV_SIDE) * KV_SIDE + (y + o % KV_SIDE) % KV_SIDE

    def behind(o):
        return ((z + KV_SIDE - o // KV_SIDE) % KV_SIDE) * KV_SIDE + (y + KV_SIDE - o % KV_SIDE) % KV_SIDE

    def tp_ahead(u):
        return ((x + u // 2) % 4) * 2 + (core + u) % 2

    def remote(kind, j, src, dst, device):
        return pltpu.make_async_remote_copy(
            src_ref=src, dst_ref=dst, send_sem=send_sem.at[kind, j], recv_sem=recv_sem.at[kind, j],
            device_id=device, device_id_type=MESH,
        )

    def arrived(kind, j, ref):
        remote(kind, j, ref, ref, {"kv": ahead(1)}).wait_recv()

    def gone(kind, j, ref):
        remote(kind, j, ref, ref, {"kv": ahead(1)}).wait_send()

    def others(ref, j):
        return ref.at[pl.ds(j * N_KV + 1, N_KV - 1)]

    barrier = pltpu.get_barrier_semaphore()
    for o in range(1, N_KV):
        pl.semaphore_signal(barrier, inc=1, device_id={"kv": ahead(o)}, device_id_type=MESH)
    for u in range(1, N_TP):
        pl.semaphore_signal(barrier, inc=1, device_id={"tp": tp_ahead(u)}, device_id_type=MESH)

    wf_copy = pltpu.make_async_copy(w_forget.at[:, pl.ds(kv * 256, 256)], wf, local_sem.at[0])
    gate_copy = pltpu.make_async_copy(gate_sums, gates, local_sem.at[1])
    key_copy = pltpu.make_async_copy(key_cache, keys, local_sem.at[2])
    value_copy = pltpu.make_async_copy(value_cache, values.at[:, pl.ds(0, head_dim)], local_sem.at[3])
    wf_copy.start()
    gate_copy.start()
    key_copy.start()
    value_copy.start()

    w_kv[...] = jnp.concatenate([w_key[...].astype(f32), w_value[...].astype(f32)], axis=0).astype(bf16)
    wf_copy.wait()
    gate_copy.wait()
    pick = (lanes((8, 32)) == rows_of((8, 32)) + 4 * tp) & (rows_of((8, 32)) < 4)
    gate_weights = dot(pick.astype(f32).astype(bf16), wf[...]).astype(bf16)
    square_row = (rows_of((8, 256)) == 4).astype(f32).astype(bf16)
    gain = norm_gain[...].astype(f32)
    gain = jnp.concatenate([gain[0:1], gain[1:2]], axis=1)
    place = lanes((heads, positions)) + kv * positions
    tile_lane = lanes((8, 128))
    tile_row = rows_of((8, 128))

    def project(o, carry):
        chunk = ahead(o)
        wide = jnp.concatenate([tokens[chunk * seqs + j].astype(f32) for j in range(seqs)], axis=0)
        wide = padded(wide, 128)
        scaled = (wide * gain).astype(bf16)
        high, low = halves(wide * wide)
        tile = dot_nt(gate_weights, scaled) + dot_nt(square_row, high) + dot_nt(square_row, low)
        for j in range(seqs):
            b = chunk * seqs + j
            last = jnp.sum(
                jnp.where(place == lengths[b] + accepted[b] - 1, gates[b], 0.0), axis=1, keepdims=True
            )
            last = jnp.concatenate([last, jnp.zeros((4, 1), f32)], axis=0)
            tile = jnp.where(tile_lane == share + j, last, tile)
        s_send[o] = tile
        projected = jnp.concatenate([dot(scaled, w_query[...]), dot_nt(scaled, w_kv[...])], axis=1)
        for j in range(seqs):
            p_send[j * N_KV + o] = projected[j * drafts : (j + 1) * drafts].astype(bf16)
        own_proj[...] = projected[:share]
        return carry

    def project_four(i, carry):
        for k in range(4):
            project(N_KV - 1 - 4 * i - k, carry)
        return carry

    lax.fori_loop(0, N_KV // 4, project_four, 0)

    pl.semaphore_wait(barrier, N_KV + N_TP - 2)
    for o in range(1, N_KV):
        remote(STAT, 0, s_send.at[o], s_recv.at[o], {"kv": ahead(o)}).start()
    for j in range(seqs):
        for o in range(1, N_KV):
            at = j * N_KV + o
            remote(PROJ, j, p_send.at[at], p_recv.at[at], {"kv": ahead(o)}).start()

    row_lane = lanes((1, 128))
    for j in range(seqs):
        for p in range(drafts):
            parent = parents[p, kv * seqs + j]
            at = jnp.where(parent >= 0, parent + drafts * j, -1)
            i = drafts * j + p
            reach[i : i + 1, :] = ((row_lane == i) | (row_lane == at)).astype(f32)
    reach[share:, :] = jnp.zeros((128 - share, 128), f32)
    closure = reach[...]
    for _ in range(5):
        closure = jnp.minimum(dot(closure.astype(bf16), closure.astype(bf16)), 1.0)
    reach[...] = closure

    def set_ones(b, carry):
        values[b, head_dim:, :] = jnp.ones((16, positions), bf16)
        return carry

    lax.fori_loop(0, values.shape[0], set_ones, 0)

    head_of = lax.broadcasted_iota(jnp.int32, (384, 384), 0) // head_dim
    head_at = lax.broadcasted_iota(jnp.int32, (384, 384), 1) // head_dim
    head_mean = jnp.where(head_of == head_at, 1.0 / head_dim, 0.0).astype(bf16)
    gains = jnp.concatenate([query_gain[...].astype(f32)] * 4 + [key_gain[...].astype(f32)] * 2, axis=1)
    q_own[share:, :] = jnp.zeros((128 - share, width), f32)
    kv_own[share:, :] = jnp.zeros((128 - share, 128), f32)

    arrived(STAT, 0, others(s_recv, 0))
    stats = s_send[0]
    for o in range(1, N_KV):
        stats = stats + s_recv[o]
    inverse_tile = lax.rsqrt(stats / model_width + eps)
    inverse = jnp.concatenate([inverse_tile] * 16, axis=0).T
    for j in range(seqs):
        rows = slice(j * drafts, (j + 1) * drafts)
        arrived(PROJ, j, others(p_recv, j))
        total = own_proj[rows, :]
        for o in range(1, N_KV):
            total = total + p_recv[j * N_KV + o].astype(f32)
        total = total * inverse[rows, 4:5]
        high, low = halves(total * total)
        mean_sq = dot(high, head_mean) + dot(low, head_mean)
        normed = total * lax.rsqrt(mean_sq + eps) * gains
        query = normed[:, :width].astype(bf16).astype(f32) * head_dim ** (-0.5)
        q_all[j * N_KV] = query.astype(bf16)
        for o in range(1, N_KV):
            remote(QUERY, j, q_all.at[j * N_KV], q_all.at[j * N_KV + o], {"kv": ahead(o)}).start()
        q_own[rows, :] = query
        kv_own[rows, :] = jnp.concatenate(
            [normed[:, width : width + head_dim], total[:, width + head_dim :]], axis=1
        )

    bias = jnp.where(
        tile_row == 0, forget_bias[0],
        jnp.where(tile_row == 1, forget_bias[1], jnp.where(tile_row == 2, forget_bias[2], forget_bias[3])),
    )
    gate_pre = stats * inverse_tile[4:5, :] + bias
    log_gate = jnp.minimum(gate_pre, 0.0) - jnp.log1p(jnp.exp(-jnp.abs(gate_pre)))
    log_gate = jnp.where(tile_lane < share, log_gate, 0.0)
    top_part = log_gate.astype(bf16)
    middle, last_part = halves(log_gate - top_part.astype(f32))
    follows = reach[...].astype(bf16)
    path = dot_nt(top_part, follows) + dot_nt(middle, follows) + dot_nt(last_part, follows)
    last_gate = jnp.where(
        tile_lane < drafts, stats[:, share : share + 1],
        jnp.where(tile_lane < 2 * drafts, stats[:, share + 1 : share + 2], stats[:, share + 2 : share + 3]),
    )
    bias_tile = path + last_gate

    wide_lane = lanes((heads * drafts, 128))
    own_queries = q_own[...]
    k_own = kv_own[:, :head_dim].astype(bf16)
    v_own = kv_own[:, head_dim:].astype(bf16)
    seen = reach[...] > 0.5
    new_parts, new_sums = [], []
    for h in range(heads):
        logits = dot_nt(own_queries[:, h * head_dim : (h + 1) * head_dim].astype(bf16), k_own)
        logits = jnp.where(seen, logits - bias_tile[h : h + 1, :], floor_value)
        top = jnp.max(logits, axis=1, keepdims=True)
        weight = jnp.where(seen, jnp.exp(logits - top), 0.0)
        total_new = jnp.sum(weight, axis=1, keepdims=True)
        new_parts.append((dot(weight.astype(bf16), v_own) / total_new)[:share])
        new_sums.append(top + jnp.log(total_new))
    new_out[...] = jnp.concatenate(new_parts, axis=1)
    columns = jnp.zeros((heads * drafts, 128), f32)
    for j in range(seqs):
        column = jnp.concatenate([s[j * drafts : (j + 1) * drafts] for s in new_sums], axis=0)
        columns = jnp.where(wide_lane == j, column, columns)
    new_tile[...] = padded(columns, 128).T[:8]

    key_copy.wait()
    value_copy.wait()

    def attend(j, o, sums):
        src = behind(o)
        b = src * seqs + j
        at = j * N_KV + o
        block = q_all[at].astype(f32)
        stacked = jnp.concatenate(
            [block[:, h * head_dim : (h + 1) * head_dim] for h in range(heads)], axis=0
        ).astype(bf16)
        logits = dot(stacked, keys[b])
        kept = jnp.where(place < lengths[b] + accepted[b], -gates[b], floor_value)
        tops, weights = [], []
        for h in range(heads):
            row = logits[h * drafts : (h + 1) * drafts] + kept[h : h + 1]
            top = jnp.max(row, axis=1, keepdims=True)
            tops.append(top)
            weights.append(jnp.exp(row - top))
        weighted = dot_nt(jnp.concatenate(weights, axis=0).astype(bf16), values[b])
        total = weighted[:, head_dim : head_dim + 1]
        weighted = weighted[:, :head_dim] / total
        o_send[at] = jnp.concatenate(
            [weighted[h * drafts : (h + 1) * drafts] for h in range(heads)], axis=1
        ).astype(bf16)
        return jnp.where(wide_lane == o, jnp.concatenate(tops, axis=0) + jnp.log(total), sums)

    def attend_all(j, first, last, sums):
        for start, stop in GROUPS:
            if start < first or stop > last:
                continue
            if start == 1:
                arrived(QUERY, j, others(q_all, j))
            for o in range(start, stop):
                sums = attend(j, o, sums)
            for o in range(max(start, 1), stop):
                at = j * N_KV + o
                remote(PART, j, o_send.at[at], o_recv.at[at], {"kv": behind(o)}).start()
        if last < N_KV:
            return sums
        table = padded(sums, 128).T
        l_recv[j * N_KV] = table[:1]
        for o in range(1, N_KV):
            at = j * N_KV + o
            l_send[at] = table[o : o + 1]
        for o in range(1, N_KV):
            at = j * N_KV + o
            remote(LSE, j, l_send.at[at], l_recv.at[at], {"kv": behind(o)}).start()
        return sums

    low_half = lanes((drafts, 128)) < head_dim

    def merge(j):
        arrived(LSE, j, others(l_recv, j))
        table = jnp.concatenate([l_recv[j * N_KV + o] for o in range(N_KV)], axis=0)
        new = new_tile[j : j + 1, :]
        top = jnp.maximum(jnp.max(table, axis=0, keepdims=True), new)
        factors = jnp.exp(table - top)
        factor_new = jnp.exp(new - top)
        whole = jnp.sum(factors, axis=0, keepdims=True) + factor_new
        spread = padded(jnp.concatenate([factors / whole, padded(factor_new / whole, 8)], axis=0), 128).T

        def factor_rows(at):
            column = spread[:, at : at + 1]
            return jnp.concatenate(
                [
                    jnp.where(
                        low_half,
                        column[2 * g * drafts : (2 * g + 1) * drafts],
                        column[(2 * g + 1) * drafts : (2 * g + 2) * drafts],
                    )
                    for g in range(2)
                ],
                axis=1,
            )

        merged = new_out[j * drafts : (j + 1) * drafts, :] * factor_rows(N_KV)
        merged = merged + o_send[j * N_KV].astype(f32) * factor_rows(0)
        arrived(PART, j, others(o_recv, j))
        for o in range(1, N_KV):
            merged = merged + o_recv[j * N_KV + o].astype(f32) * factor_rows(o)
        a_all[j * N_KV] = merged.astype(bf16)
        for o in range(1, N_KV):
            remote(ATT, j, a_all.at[j * N_KV], a_all.at[j * N_KV + o], {"kv": ahead(o)}).start()

    def output(j):
        arrived(ATT, j, others(a_all, j))
        rows = jnp.concatenate([a_all[j * N_KV + o].astype(f32) for o in range(N_KV)], axis=0).astype(bf16)
        part = dot(rows, w_out[...])
        for o in range(N_KV):
            t_send[j * N_KV + o] = part[o * drafts : (o + 1) * drafts].astype(bf16)
        for u in range(N_TP):
            owner = tp_ahead(u)
            for half in range(2):
                chunk = owner * 2 + half
                o = ((z + 4 - chunk // 4) % 4) * 4 + (y + 4 - chunk % 4) % 4
                at = j * N_KV + u * 2 + half
                if u == 0:
                    t_recv[at] = t_send[j * N_KV + o]
                else:
                    remote(OUT, j, t_send.at[j * N_KV + o], t_recv.at[at], {"tp": owner}).start()

    def add_up(j):
        arrived(OUT, j, t_recv.at[pl.ds(j * N_KV + 2, N_KV - 2)])
        for half in range(2):
            summed = t_recv[j * N_KV + half].astype(f32)
            for u in range(1, N_TP):
                summed = summed + t_recv[j * N_KV + u * 2 + half].astype(f32)
            seq = (tp * 2 + half) * seqs + j
            fin[j * 2 + half] = summed.astype(bf16)
            for u in range(1, N_TP):
                remote(FINAL, j, fin.at[j * 2 + half], out.at[seq], {"tp": tp_ahead(u)}).start()
            out[seq] = summed.astype(bf16)

    none = jnp.zeros((heads * drafts, 128), f32)
    attend_all(0, 0, N_KV, none)
    attend_all(1, 0, N_KV, none)
    merge(0)
    sums = attend_all(2, 0, 11, none)
    merge(1)
    attend_all(2, 11, N_KV, sums)
    output(0)
    merge(2)
    output(1)
    add_up(0)
    output(2)
    add_up(1)
    add_up(2)
    for j in range(seqs):
        arrived(FINAL, j, t_recv.at[pl.ds(j * N_KV + 2, N_KV - 2)])
    gone(STAT, 0, others(s_send, 0))
    for j in range(seqs):
        gone(PROJ, j, others(p_send, j))
        gone(QUERY, j, others(q_all, j))
        gone(PART, j, others(o_send, j))
        gone(LSE, j, others(l_send, j))
        gone(ATT, j, others(a_all, j))
        gone(OUT, j, t_send.at[pl.ds(j * N_KV + 2, N_KV - 2)])
        gone(FINAL, j, t_send.at[pl.ds(j * N_KV + 2, N_KV - 2)])


def body(
    tokens, norm_gain, w_query, w_key, w_value, w_forget, forget_bias, query_gain, key_gain, w_out,
    key_cache, value_cache, gate_sums, parents, lengths, accepted,
):
    seq_count, drafts, local_width = tokens.shape
    share = seq_count * drafts // N_KV
    vmem = pl.BlockSpec(memory_space=pltpu.VMEM)
    smem = pl.BlockSpec(memory_space=pltpu.SMEM)
    anywhere = pl.BlockSpec(memory_space=pl.ANY)
    mixed = pl.pallas_call(
        kernel,
        out_shape=pltpu.VMEM(tokens.shape, bf16),
        in_specs=[
            vmem, vmem, vmem, vmem, vmem, anywhere, smem, vmem, vmem, vmem,
            anywhere, anywhere, anywhere, smem, smem, smem,
        ],
        out_specs=vmem,
        scratch_shapes=[
            pltpu.VMEM((128, local_width), bf16),
            pltpu.VMEM((w_forget.shape[1], local_width), bf16),
            pltpu.VMEM(key_cache.shape, bf16),
            pltpu.VMEM((seq_count, value_cache.shape[1] + 16, value_cache.shape[2]), bf16),
            pltpu.VMEM(gate_sums.shape, f32),
            pltpu.VMEM((128, 128), f32),
            pltpu.VMEM((seq_count, drafts, 384), bf16),
            pltpu.VMEM((seq_count, drafts, 384), bf16),
            pltpu.VMEM((N_KV, 8, 128), f32),
            pltpu.VMEM((N_KV, 8, 128), f32),
            pltpu.VMEM((share, 384), f32),
            pltpu.VMEM((seq_count, drafts, 256), bf16),
            pltpu.VMEM((128, 256), f32),
            pltpu.VMEM((128, 128), f32),
            pltpu.VMEM((share, 256), f32),
            pltpu.VMEM((8, 128), f32),
            pltpu.VMEM((seq_count, drafts, 256), bf16),
            pltpu.VMEM((seq_count, drafts, 256), bf16),
            pltpu.VMEM((seq_count, 1, 128), f32),
            pltpu.VMEM((seq_count, 1, 128), f32),
            pltpu.VMEM((seq_count, drafts, 256), bf16),
            pltpu.VMEM((seq_count, drafts, 256), bf16),
            pltpu.VMEM((seq_count, drafts, 256), bf16),
            pltpu.VMEM((6, drafts, 256), bf16),
            pltpu.SemaphoreType.DMA((10,)),
            pltpu.SemaphoreType.DMA((8, 3)),
            pltpu.SemaphoreType.DMA((8, 3)),
        ],
        compiler_params=pltpu.CompilerParams(
            collective_id=0, has_side_effects=True, vmem_limit_bytes=66350000
        ),
        name="tree_attention",
    )(
        tokens, norm_gain.reshape(2, -1), w_query, w_key.T, w_value.T, w_forget.T,
        forget_bias, query_gain.reshape(1, -1), key_gain.reshape(1, -1), w_out,
        key_cache, value_cache, gate_sums, parents.T, lengths, accepted,
    )
    return mixed


def solution(mesh):
    return jax.shard_map(
        body,
        mesh=mesh,
        in_specs=(
            P(None, None, "kv"),
            P("kv"),
            P("kv", "tp"),
            P("kv", "tp"),
            P("kv", "tp"),
            P(),
            P("tp"),
            P(),
            P(),
            P("tp", "kv"),
            P(None, "tp", "kv"),
            P(None, "tp", "kv"),
            P(None, "tp", "kv"),
            P(),
            P(),
            P(),
        ),
        out_specs=P(None, None, "kv"),
        check_vma=False,
    )
```

```python
import functools

import jax
import jax.numpy as jnp
from jax import lax
from jax.experimental import pallas as pl
from jax.experimental.pallas import tpu as pltpu
from jax.sharding import PartitionSpec as P

f32, bf16 = jnp.float32, jnp.bfloat16
eps = 1e-05
floor_value = -1e30
KV_SIDE = 4
N_KV = 16
N_TP = 8
GROUPS = ((0, 1), (1, 6), (6, 12), (12, 16))
MESH = pl.DeviceIdType.MESH

PROJ, STAT, QUERY, PART, LSE, ATT, OUT, FINAL = range(8)


def dot(a, b):
    return jnp.dot(a, b, preferred_element_type=f32)


def dot_nt(a, b):
    return lax.dot_general(a, b, (((1,), (1,)), ((), ())), preferred_element_type=f32)


def halves(value):
    high = value.astype(bf16)
    return high, (value - high.astype(f32)).astype(bf16)


def padded(value, rows):
    return jnp.concatenate([value, jnp.zeros((rows - value.shape[0], value.shape[1]), value.dtype)], axis=0)


def lanes(shape):
    return lax.broadcasted_iota(jnp.int32, shape, 1)


def rows_of(shape):
    return lax.broadcasted_iota(jnp.int32, shape, 0)


def kernel(
    tokens, norm_gain, w_query, w_key, w_value, w_forget, forget_bias, query_gain, key_gain, w_out,
    key_cache, value_cache, gate_sums, parents, lengths, accepted,
    out,
    w_kv, wf, keys, values, gates, reach, p_send, p_recv, s_send, s_recv, own_proj, q_all, q_own, kv_own,
    new_out, new_tile, o_send, o_recv, l_send, l_recv, a_all, t_send, t_recv, fin,
    local_sem, send_sem, recv_sem,
):
    kv = lax.axis_index("kv")
    tp = lax.axis_index("tp")
    z, y = kv // KV_SIDE, kv % KV_SIDE
    x, core = tp // 2, tp % 2
    seqs = 3
    drafts = tokens.shape[1]
    share = seqs * drafts
    heads = 4
    head_dim = 64
    width = heads * head_dim
    positions = key_cache.shape[2]
    model_width = w_forget.shape[1]

    def ahead(o):
        return ((z + o // KV_SIDE) % KV_SIDE) * KV_SIDE + (y + o % KV_SIDE) % KV_SIDE

    def behind(o):
        return ((z + KV_SIDE - o // KV_SIDE) % KV_SIDE) * KV_SIDE + (y + KV_SIDE - o % KV_SIDE) % KV_SIDE

    def tp_ahead(u):
        return ((x + u // 2) % 4) * 2 + (core + u) % 2

    def remote(kind, j, src, dst, device):
        return pltpu.make_async_remote_copy(
            src_ref=src, dst_ref=dst, send_sem=send_sem.at[kind, j], recv_sem=recv_sem.at[kind, j],
            device_id=device, device_id_type=MESH,
        )

    def arrived(kind, j, ref):
        remote(kind, j, ref, ref, {"kv": ahead(1)}).wait_recv()

    def gone(kind, j, ref):
        remote(kind, j, ref, ref, {"kv": ahead(1)}).wait_send()

    def others(ref, j):
        return ref.at[pl.ds(j * N_KV + 1, N_KV - 1)]

    barrier = pltpu.get_barrier_semaphore()
    for o in range(1, N_KV):
        pl.semaphore_signal(barrier, inc=1, device_id={"kv": ahead(o)}, device_id_type=MESH)
    for u in range(1, N_TP):
        pl.semaphore_signal(barrier, inc=1, device_id={"tp": tp_ahead(u)}, device_id_type=MESH)

    wf_copy = pltpu.make_async_copy(w_forget.at[:, pl.ds(kv * 256, 256)], wf, local_sem.at[0])
    gate_copy = pltpu.make_async_copy(gate_sums, gates, local_sem.at[1])
    key_copy = pltpu.make_async_copy(key_cache, keys, local_sem.at[2])
    value_copy = pltpu.make_async_copy(value_cache, values.at[:, pl.ds(0, head_dim)], local_sem.at[3])
    wf_copy.start()
    gate_copy.start()
    key_copy.start()
    value_copy.start()

    w_kv[...] = jnp.concatenate([w_key[...].astype(f32), w_value[...].astype(f32)], axis=0).astype(bf16)
    wf_copy.wait()
    gate_copy.wait()
    pick = (lanes((8, 32)) == rows_of((8, 32)) + 4 * tp) & (rows_of((8, 32)) < 4)
    gate_weights = dot(pick.astype(f32).astype(bf16), wf[...]).astype(bf16)
    square_row = (rows_of((8, 256)) == 4).astype(f32).astype(bf16)
    gain = norm_gain[...].astype(f32)
    gain = jnp.concatenate([gain[0:1], gain[1:2]], axis=1)
    place = lanes((heads, positions)) + kv * positions
    tile_lane = lanes((8, 128))
    tile_row = rows_of((8, 128))

    def project(o, carry):
        chunk = ahead(o)
        wide = jnp.concatenate([tokens[chunk * seqs + j].astype(f32) for j in range(seqs)], axis=0)
        wide = padded(wide, 128)
        scaled = (wide * gain).astype(bf16)
        high, low = halves(wide * wide)
        tile = dot_nt(gate_weights, scaled) + dot_nt(square_row, high) + dot_nt(square_row, low)
        for j in range(seqs):
            b = chunk * seqs + j
            last = jnp.sum(
                jnp.where(place == lengths[b] + accepted[b] - 1, gates[b], 0.0), axis=1, keepdims=True
            )
            last = jnp.concatenate([last, jnp.zeros((4, 1), f32)], axis=0)
            tile = jnp.where(tile_lane == share + j, last, tile)
        s_send[o] = tile
        projected = jnp.concatenate([dot(scaled, w_query[...]), dot_nt(scaled, w_kv[...])], axis=1)
        for j in range(seqs):
            p_send[j * N_KV + o] = projected[j * drafts : (j + 1) * drafts].astype(bf16)
        own_proj[...] = projected[:share]
        return carry

    def project_four(i, carry):
        for k in range(4):
            project(N_KV - 1 - 4 * i - k, carry)
        return carry

    lax.fori_loop(0, N_KV // 4, project_four, 0)

    pl.semaphore_wait(barrier, N_KV + N_TP - 2)
    for o in range(1, N_KV):
        remote(STAT, 0, s_send.at[o], s_recv.at[o], {"kv": ahead(o)}).start()
    for j in range(seqs):
        for o in range(1, N_KV):
            at = j * N_KV + o
            remote(PROJ, j, p_send.at[at], p_recv.at[at], {"kv": ahead(o)}).start()

    row_lane = lanes((1, 128))
    for j in range(seqs):
        for p in range(drafts):
            parent = parents[p, kv * seqs + j]
            at = jnp.where(parent >= 0, parent + drafts * j, -1)
            i = drafts * j + p
            reach[i : i + 1, :] = ((row_lane == i) | (row_lane == at)).astype(f32)
    reach[share:, :] = jnp.zeros((128 - share, 128), f32)
    closure = reach[...]
    for _ in range(5):
        closure = jnp.minimum(dot(closure.astype(bf16), closure.astype(bf16)), 1.0)
    reach[...] = closure

    def set_ones(b, carry):
        values[b, head_dim:, :] = jnp.ones((16, positions), bf16)
        return carry

    lax.fori_loop(0, values.shape[0], set_ones, 0)

    head_of = lax.broadcasted_iota(jnp.int32, (384, 384), 0) // head_dim
    head_at = lax.broadcasted_iota(jnp.int32, (384, 384), 1) // head_dim
    head_mean = jnp.where(head_of == head_at, 1.0 / head_dim, 0.0).astype(bf16)
    gains = jnp.concatenate([query_gain[...].astype(f32)] * 4 + [key_gain[...].astype(f32)] * 2, axis=1)
    q_own[share:, :] = jnp.zeros((128 - share, width), f32)
    kv_own[share:, :] = jnp.zeros((128 - share, 128), f32)

    arrived(STAT, 0, others(s_recv, 0))
    stats = s_send[0]
    for o in range(1, N_KV):
        stats = stats + s_recv[o]
    inverse_tile = lax.rsqrt(stats / model_width + eps)
    inverse = jnp.concatenate([inverse_tile] * 16, axis=0).T
    for j in range(seqs):
        rows = slice(j * drafts, (j + 1) * drafts)
        arrived(PROJ, j, others(p_recv, j))
        total = own_proj[rows, :]
        for o in range(1, N_KV):
            total = total + p_recv[j * N_KV + o].astype(f32)
        total = total * inverse[rows, 4:5]
        high, low = halves(total * total)
        mean_sq = dot(high, head_mean) + dot(low, head_mean)
        normed = total * lax.rsqrt(mean_sq + eps) * gains
        query = normed[:, :width].astype(bf16).astype(f32) * head_dim ** (-0.5)
        q_all[j * N_KV] = query.astype(bf16)
        for o in range(1, N_KV):
            remote(QUERY, j, q_all.at[j * N_KV], q_all.at[j * N_KV + o], {"kv": ahead(o)}).start()
        q_own[rows, :] = query
        kv_own[rows, :] = jnp.concatenate(
            [normed[:, width : width + head_dim], total[:, width + head_dim :]], axis=1
        )

    bias = jnp.where(
        tile_row == 0, forget_bias[0],
        jnp.where(tile_row == 1, forget_bias[1], jnp.where(tile_row == 2, forget_bias[2], forget_bias[3])),
    )
    gate_pre = stats * inverse_tile[4:5, :] + bias
    log_gate = jnp.minimum(gate_pre, 0.0) - jnp.log1p(jnp.exp(-jnp.abs(gate_pre)))
    log_gate = jnp.where(tile_lane < share, log_gate, 0.0)
    top_part = log_gate.astype(bf16)
    middle, last_part = halves(log_gate - top_part.astype(f32))
    follows = reach[...].astype(bf16)
    path = dot_nt(top_part, follows) + dot_nt(middle, follows) + dot_nt(last_part, follows)
    last_gate = jnp.where(
        tile_lane < drafts, stats[:, share : share + 1],
        jnp.where(tile_lane < 2 * drafts, stats[:, share + 1 : share + 2], stats[:, share + 2 : share + 3]),
    )
    bias_tile = path + last_gate

    wide_lane = lanes((heads * drafts, 128))
    own_queries = q_own[...]
    k_own = kv_own[:, :head_dim].astype(bf16)
    v_own = kv_own[:, head_dim:].astype(bf16)
    seen = reach[...] > 0.5
    new_parts, new_sums = [], []
    for h in range(heads):
        logits = dot_nt(own_queries[:, h * head_dim : (h + 1) * head_dim].astype(bf16), k_own)
        logits = jnp.where(seen, logits - bias_tile[h : h + 1, :], floor_value)
        top = jnp.max(logits, axis=1, keepdims=True)
        weight = jnp.where(seen, jnp.exp(logits - top), 0.0)
        total_new = jnp.sum(weight, axis=1, keepdims=True)
        new_parts.append((dot(weight.astype(bf16), v_own) / total_new)[:share])
        new_sums.append(top + jnp.log(total_new))
    new_out[...] = jnp.concatenate(new_parts, axis=1)
    columns = jnp.zeros((heads * drafts, 128), f32)
    for j in range(seqs):
        column = jnp.concatenate([s[j * drafts : (j + 1) * drafts] for s in new_sums], axis=0)
        columns = jnp.where(wide_lane == j, column, columns)
    new_tile[...] = padded(columns, 128).T[:8]

    key_copy.wait()
    value_copy.wait()

    def attend(j, o, sums):
        src = behind(o)
        b = src * seqs + j
        at = j * N_KV + o
        block = q_all[at].astype(f32)
        stacked = jnp.concatenate(
            [block[:, h * head_dim : (h + 1) * head_dim] for h in range(heads)], axis=0
        ).astype(bf16)
        logits = dot(stacked, keys[b])
        kept = jnp.where(place < lengths[b] + accepted[b], -gates[b], floor_value)
        tops, weights = [], []
        for h in range(heads):
            row = logits[h * drafts : (h + 1) * drafts] + kept[h : h + 1]
            top = jnp.max(row, axis=1, keepdims=True)
            tops.append(top)
            weights.append(jnp.exp(row - top))
        weighted = dot_nt(jnp.concatenate(weights, axis=0).astype(bf16), values[b])
        total = weighted[:, head_dim : head_dim + 1]
        weighted = weighted[:, :head_dim] / total
        o_send[at] = jnp.concatenate(
            [weighted[h * drafts : (h + 1) * drafts] for h in range(heads)], axis=1
        ).astype(bf16)
        return jnp.where(wide_lane == o, jnp.concatenate(tops, axis=0) + jnp.log(total), sums)

    def attend_all(j, first, last, sums):
        for start, stop in GROUPS:
            if start < first or stop > last:
                continue
            if start == 1:
                arrived(QUERY, j, others(q_all, j))
            for o in range(start, stop):
                sums = attend(j, o, sums)
            for o in range(max(start, 1), stop):
                at = j * N_KV + o
                remote(PART, j, o_send.at[at], o_recv.at[at], {"kv": behind(o)}).start()
        if last < N_KV:
            return sums
        table = padded(sums, 128).T
        l_recv[j * N_KV] = table[:1]
        for o in range(1, N_KV):
            at = j * N_KV + o
            l_send[at] = table[o : o + 1]
        for o in range(1, N_KV):
            at = j * N_KV + o
            remote(LSE, j, l_send.at[at], l_recv.at[at], {"kv": behind(o)}).start()
        return sums

    low_half = lanes((drafts, 128)) < head_dim

    def merge(j):
        arrived(LSE, j, others(l_recv, j))
        table = jnp.concatenate([l_recv[j * N_KV + o] for o in range(N_KV)], axis=0)
        new = new_tile[j : j + 1, :]
        top = jnp.maximum(jnp.max(table, axis=0, keepdims=True), new)
        factors = jnp.exp(table - top)
        factor_new = jnp.exp(new - top)
        whole = jnp.sum(factors, axis=0, keepdims=True) + factor_new
        spread = padded(jnp.concatenate([factors / whole, padded(factor_new / whole, 8)], axis=0), 128).T

        def factor_rows(at):
            column = spread[:, at : at + 1]
            return jnp.concatenate(
                [
                    jnp.where(
                        low_half,
                        column[2 * g * drafts : (2 * g + 1) * drafts],
                        column[(2 * g + 1) * drafts : (2 * g + 2) * drafts],
                    )
                    for g in range(2)
                ],
                axis=1,
            )

        merged = new_out[j * drafts : (j + 1) * drafts, :] * factor_rows(N_KV)
        merged = merged + o_send[j * N_KV].astype(f32) * factor_rows(0)
        arrived(PART, j, others(o_recv, j))
        for o in range(1, N_KV):
            merged = merged + o_recv[j * N_KV + o].astype(f32) * factor_rows(o)
        a_all[j * N_KV] = merged.astype(bf16)
        for o in range(1, N_KV):
            remote(ATT, j, a_all.at[j * N_KV], a_all.at[j * N_KV + o], {"kv": ahead(o)}).start()

    def output(j):
        arrived(ATT, j, others(a_all, j))
        rows = jnp.concatenate([a_all[j * N_KV + o].astype(f32) for o in range(N_KV)], axis=0).astype(bf16)
        part = dot(rows, w_out[...])
        for o in range(N_KV):
            t_send[j * N_KV + o] = part[o * drafts : (o + 1) * drafts].astype(bf16)
        for u in range(N_TP):
            owner = tp_ahead(u)
            for half in range(2):
                chunk = owner * 2 + half
                o = ((z + 4 - chunk // 4) % 4) * 4 + (y + 4 - chunk % 4) % 4
                at = j * N_KV + u * 2 + half
                if u == 0:
                    t_recv[at] = t_send[j * N_KV + o]
                else:
                    remote(OUT, j, t_send.at[j * N_KV + o], t_recv.at[at], {"tp": owner}).start()

    def add_up(j):
        arrived(OUT, j, t_recv.at[pl.ds(j * N_KV + 2, N_KV - 2)])
        for half in range(2):
            summed = t_recv[j * N_KV + half].astype(f32)
            for u in range(1, N_TP):
                summed = summed + t_recv[j * N_KV + u * 2 + half].astype(f32)
            seq = (tp * 2 + half) * seqs + j
            fin[j * 2 + half] = summed.astype(bf16)
            for u in range(1, N_TP):
                remote(FINAL, j, fin.at[j * 2 + half], out.at[seq], {"tp": tp_ahead(u)}).start()
            out[seq] = summed.astype(bf16)

    none = jnp.zeros((heads * drafts, 128), f32)
    attend_all(0, 0, N_KV, none)
    attend_all(1, 0, N_KV, none)
    merge(0)
    attend_all(2, 0, N_KV, none)
    merge(1)
    output(0)
    merge(2)
    output(1)
    add_up(0)
    output(2)
    add_up(1)
    add_up(2)
    for j in range(seqs):
        arrived(FINAL, j, t_recv.at[pl.ds(j * N_KV + 2, N_KV - 2)])
    gone(STAT, 0, others(s_send, 0))
    for j in range(seqs):
        gone(PROJ, j, others(p_send, j))
        gone(QUERY, j, others(q_all, j))
        gone(PART, j, others(o_send, j))
        gone(LSE, j, others(l_send, j))
        gone(ATT, j, others(a_all, j))
        gone(OUT, j, t_send.at[pl.ds(j * N_KV + 2, N_KV - 2)])
        gone(FINAL, j, t_send.at[pl.ds(j * N_KV + 2, N_KV - 2)])


def body(
    tokens, norm_gain, w_query, w_key, w_value, w_forget, forget_bias, query_gain, key_gain, w_out,
    key_cache, value_cache, gate_sums, parents, lengths, accepted,
):
    seq_count, drafts, local_width = tokens.shape
    share = seq_count * drafts // N_KV
    vmem = pl.BlockSpec(memory_space=pltpu.VMEM)
    smem = pl.BlockSpec(memory_space=pltpu.SMEM)
    anywhere = pl.BlockSpec(memory_space=pl.ANY)
    mixed = pl.pallas_call(
        kernel,
        out_shape=pltpu.VMEM(tokens.shape, bf16),
        in_specs=[
            vmem, vmem, vmem, vmem, vmem, anywhere, smem, vmem, vmem, vmem,
            anywhere, anywhere, anywhere, smem, smem, smem,
        ],
        out_specs=vmem,
        scratch_shapes=[
            pltpu.VMEM((128, local_width), bf16),
            pltpu.VMEM((w_forget.shape[1], local_width), bf16),
            pltpu.VMEM(key_cache.shape, bf16),
            pltpu.VMEM((seq_count, value_cache.shape[1] + 16, value_cache.shape[2]), bf16),
            pltpu.VMEM(gate_sums.shape, f32),
            pltpu.VMEM((128, 128), f32),
            pltpu.VMEM((seq_count, drafts, 384), bf16),
            pltpu.VMEM((seq_count, drafts, 384), bf16),
            pltpu.VMEM((N_KV, 8, 128), f32),
            pltpu.VMEM((N_KV, 8, 128), f32),
            pltpu.VMEM((share, 384), f32),
            pltpu.VMEM((seq_count, drafts, 256), bf16),
            pltpu.VMEM((128, 256), f32),
            pltpu.VMEM((128, 128), f32),
            pltpu.VMEM((share, 256), f32),
            pltpu.VMEM((8, 128), f32),
            pltpu.VMEM((seq_count, drafts, 256), bf16),
            pltpu.VMEM((seq_count, drafts, 256), bf16),
            pltpu.VMEM((seq_count, 1, 128), f32),
            pltpu.VMEM((seq_count, 1, 128), f32),
            pltpu.VMEM((seq_count, drafts, 256), bf16),
            pltpu.VMEM((seq_count, drafts, 256), bf16),
            pltpu.VMEM((seq_count, drafts, 256), bf16),
            pltpu.VMEM((6, drafts, 256), bf16),
            pltpu.SemaphoreType.DMA((10,)),
            pltpu.SemaphoreType.DMA((8, 3)),
            pltpu.SemaphoreType.DMA((8, 3)),
        ],
        compiler_params=pltpu.CompilerParams(
            collective_id=0, has_side_effects=True, vmem_limit_bytes=66350000
        ),
        name="tree_attention",
    )(
        tokens, norm_gain.reshape(2, -1), w_query, w_key.T, w_value.T, w_forget.T,
        forget_bias, query_gain.reshape(1, -1), key_gain.reshape(1, -1), w_out,
        key_cache, value_cache, gate_sums, parents.T, lengths, accepted,
    )
    return mixed


def solution(mesh):
    return jax.shard_map(
        body,
        mesh=mesh,
        in_specs=(
            P(None, None, "kv"),
            P("kv"),
            P("kv", "tp"),
            P("kv", "tp"),
            P("kv", "tp"),
            P(),
            P("tp"),
            P(),
            P(),
            P("tp", "kv"),
            P(None, "tp", "kv"),
            P(None, "tp", "kv"),
            P(None, "tp", "kv"),
            P(),
            P(),
            P(),
        ),
        out_specs=P(None, None, "kv"),
        check_vma=False,
    )
```
